128 devices in a mesh: sp: 16 (over z, x), tp: 8 (over y, core).
Axes of the slice: x: 4, y: 4, z: 4, core: 2. Of those that a mesh axis runs over, the one named last changes fastest.
Arguments:
- tokens: bfloat16 [12288, 2048], P('sp', 'tp'), may hold values from -23 to 23, as said below
- norm_gain: float32 [2048], replicated, may hold values from 0.8 to 8, as said below
- window_query: bfloat16 [2048, 1024], P(None, 'tp'), may hold values from -0.125 to 0.125
- window_key: bfloat16 [2048, 512], P(None, 'tp'), may hold values from -0.125 to 0.125
- window_value: bfloat16 [2048, 512], P(None, 'tp'), may hold values from -0.125 to 0.125
- sink_logit: float32 [16], P('tp'), may hold values from 2 to 6
- down_query: bfloat16 [2048, 768], replicated, may hold values from -0.125 to 0.125
- down_latent: bfloat16 [2048, 512], replicated, may hold values from -0.125 to 0.125
- rotary_proj: bfloat16 [2048, 32], replicated, may hold values from -0.125 to 0.125
- query_gain: float32 [768], replicated, may hold values from 0.8 to 8, as said below
- latent_gain: float32 [512], replicated, may hold values from 0.8 to 8, as said below
- up_query: bfloat16 [768, 1536], P(None, 'tp'), may hold values from -0.21875 to 0.21875
- up_key: bfloat16 [512, 1024], P(None, 'tp'), may hold values from -0.25 to 0.25
- up_value: bfloat16 [512, 1024], P(None, 'tp'), may hold values from -0.25 to 0.25
- window_out: bfloat16 [1024, 2048], P('tp'), may hold values from -0.125 to 0.125
- latent_out: bfloat16 [1024, 2048], P('tp'), may hold values from -0.125 to 0.125
Outputs:
- mixed: bfloat16 [12288, 2048], P(('sp', 'tp'))
The draws below stay inside these ranges and needn't reach their ends.
Inputs may be any that keep to these rules, and one draw needn't show every extreme that they name: `tokens`: real-valued; the channels carry scales that vary smoothly by a factor of up to twenty across the width. `norm_gain`: positive. `query_gain`: positive. `latent_gain`: positive.
All inputs are finite; a program needn't handle non-finite values.
Results may differ from the reference program's by a relative error of at most 0.04.
The reference program's roundings to bfloat16 on the way count: a program that leaves them out, or rounds other values in their place, can miss the bound.
Values may be sent and summed in bfloat16 or wider, within the bound.
A program may use at most 128 MiB of HBM per device.

```python
import jax
import jax.numpy as jnp
from jax import lax

D = 2048
A_HEADS = 16
KV_HEADS = 8
HD = 64
B_HEADS = 16
NOPE = 64
ROPE = 32
VD = 64
QRANK = 768
KVRANK = 512
WINDOW = 128
QBLOCK = 256
TOKENS = 12288
N_TP = 8


def gain_values(key, length):
    return jax.random.uniform(key, (length,), jnp.float32, 0.8, 2.4)


def draw_norm_gain(key, part):
    return gain_values(jax.random.fold_in(key, 11), D)


def draw_query_gain(key, part):
    return gain_values(jax.random.fold_in(key, 13), QRANK)


def draw_latent_gain(key, part):
    return gain_values(jax.random.fold_in(key, 17), KVRANK)


def draw_tokens(key, part):
    phase = jax.random.uniform(jax.random.fold_in(key, 3), (), jnp.float32, 0.0, 6.2831853)
    channel = jnp.arange(D, dtype=jnp.float32)
    channel_scale = jnp.exp(1.5 * jnp.cos(6.2831853 * channel / D + phase))
    base = jnp.clip(jax.random.normal(jax.random.fold_in(key, 7), (TOKENS, D), jnp.float32), -5.0, 5.0)
    return (base * channel_scale[None, :]).astype(jnp.bfloat16)


def block_scale(own_key, dims, pieces, low, top_value):
    gain, own = 1.0, jax.random.fold_in(own_key, 6)
    for axis_at, blocks in pieces:
        steps = jnp.exp(jax.random.uniform(jax.random.fold_in(own, axis_at), (blocks,), jnp.float32, low / len(pieces), top_value / len(pieces)))
        gain = gain * jnp.repeat(steps, dims[axis_at] // blocks).reshape([-1 if axis == axis_at else 1 for axis in range(len(dims))])
    return gain


def gaussian(key, extent, spread, reach, split=(), kind=jnp.bfloat16):
    array = jax.random.normal(key, extent, jnp.float32) * spread
    if len(split) > 0:
        array = block_scale(key, extent, split, -0.22, 0.18) * array
    return jnp.clip(array, min=-reach, max=reach).astype(kind)


def setup_inputs(seed: int = 0) -> dict:
    arg_keys = jax.random.split(jax.random.key(seed), 17)
    return {
        "tokens": draw_tokens(jax.random.fold_in(arg_keys[16], 71), 0),
        "norm_gain": draw_norm_gain(jax.random.fold_in(arg_keys[16], 71), 0),
        "window_query": gaussian(arg_keys[2], (D, A_HEADS * HD), D ** -0.5, 0.125, ((1, 8),)),
        "window_key": gaussian(arg_keys[3], (D, KV_HEADS * HD), D ** -0.5, 0.125, ((1, 8),)),
        "window_value": gaussian(arg_keys[4], (D, KV_HEADS * HD), D ** -0.5, 0.125, ((1, 8),)),
        "sink_logit": jnp.clip(2.0 + 4.0 * jax.random.uniform(arg_keys[5], (A_HEADS,), jnp.float32) ** block_scale(arg_keys[5], (A_HEADS,), ((0, 8),), -0.2, 0.2), 2.0, 6.0),
        "down_query": gaussian(arg_keys[6], (D, QRANK), D ** -0.5, 0.125),
        "down_latent": gaussian(arg_keys[7], (D, KVRANK), D ** -0.5, 0.125),
        "rotary_proj": gaussian(arg_keys[8], (D, ROPE), D ** -0.5, 0.125),
        "query_gain": draw_query_gain(jax.random.fold_in(arg_keys[16], 71), 0),
        "latent_gain": draw_latent_gain(jax.random.fold_in(arg_keys[16], 71), 0),
        "up_query": gaussian(arg_keys[11], (QRANK, B_HEADS * (NOPE + ROPE)), QRANK ** -0.5, 0.21875, ((1, 8),)),
        "up_key": gaussian(arg_keys[12], (KVRANK, B_HEADS * NOPE), KVRANK ** -0.5, 0.25, ((1, 8),)),
        "up_value": gaussian(arg_keys[13], (KVRANK, B_HEADS * VD), KVRANK ** -0.5, 0.25, ((1, 8),)),
        "window_out": gaussian(arg_keys[14], (A_HEADS * HD, D), (A_HEADS * HD + B_HEADS * VD) ** -0.5, 0.125, ((0, 8),)),
        "latent_out": gaussian(arg_keys[15], (B_HEADS * VD, D), (A_HEADS * HD + B_HEADS * VD) ** -0.5, 0.125, ((0, 8),)),
    }


EPS = 1e-06
THETA = 10000.0

def rotate(vector, positions):
    half_len = vector.shape[-1] // 2
    inverse = THETA ** (-jnp.arange(half_len, dtype=jnp.float32) / half_len)
    angles = positions.astype(jnp.float32)[:, None] * inverse[None, :]
    new_shape = (angles.shape[0],) + (1,) * (vector.ndim - 2) + (half_len,)
    cosine = jnp.cos(angles).reshape(new_shape)
    sine_part = jnp.sin(angles).reshape(new_shape)
    front_half = vector[..., :half_len].astype(jnp.float32)
    second = vector[..., half_len:].astype(jnp.float32)
    return jnp.concatenate([front_half * cosine - second * sine_part, second * cosine + front_half * sine_part], axis=-1)

def norm_rows(values, gain_vec):
    as_float = values.astype(jnp.float32)
    return (as_float * lax.rsqrt(lax.optimization_barrier(jnp.mean(as_float * as_float, axis=1, keepdims=True)) + EPS) * gain_vec).astype(jnp.bfloat16)

def window_attention(q_rows, key_rows, value_rows, sink_logit):
    row_count = q_rows.shape[0]
    group = A_HEADS // KV_HEADS
    padded_keys = jnp.pad(key_rows, ((WINDOW, WINDOW), (0, 0)))
    padded_values = jnp.pad(value_rows, ((WINDOW, WINDOW), (0, 0)))
    span_len = QBLOCK + 2 * WINDOW
    distance = jnp.arange(QBLOCK)[:, None] + WINDOW - jnp.arange(span_len)[None, :]
    slopes = jnp.exp2(-8.0 * (jnp.arange(A_HEADS, dtype=jnp.float32) + 1.0) / A_HEADS).reshape(KV_HEADS, group)
    sinks = sink_logit.astype(jnp.float32).reshape(KV_HEADS, group)[:, :, None, None]

    def one_block(offset):
        queries = lax.dynamic_slice_in_dim(q_rows, offset, QBLOCK, 0).astype(jnp.float32).reshape(QBLOCK, KV_HEADS, group, HD)
        key_part = lax.dynamic_slice_in_dim(padded_keys, offset, span_len, 0).astype(jnp.float32).reshape(span_len, KV_HEADS, HD)
        value_part = lax.dynamic_slice_in_dim(padded_values, offset, span_len, 0).astype(jnp.float32).reshape(span_len, KV_HEADS, HD)
        scores = jnp.einsum('qhgd,khd->hgqk', queries, key_part) * HD ** (-0.5)
        scores = scores - slopes[:, :, None, None] * jnp.abs(distance).astype(jnp.float32)
        key_pos = offset + jnp.arange(span_len, dtype=jnp.int32) - WINDOW
        valid = (jnp.abs(distance) <= WINDOW) & ((key_pos >= 0) & (key_pos < row_count))[None, :]
        scores = jnp.where(valid, scores, -jnp.inf)
        row_max = jnp.maximum(lax.optimization_barrier(jnp.max(scores, axis=3, keepdims=True)), sinks)
        weights = jnp.exp(scores - row_max)
        weights = weights / (lax.optimization_barrier(jnp.sum(weights, axis=3, keepdims=True)) + jnp.exp(sinks - row_max))
        rounded = lax.optimization_barrier(weights.astype(jnp.bfloat16)).astype(jnp.float32)
        return jnp.einsum('hgqk,khd->qhgd', rounded, value_part).astype(jnp.bfloat16).reshape(QBLOCK, A_HEADS * HD)
    offsets = (jnp.arange(row_count // QBLOCK) * QBLOCK).astype(jnp.int32)
    return lax.map(one_block, offsets).reshape(row_count, A_HEADS * HD)

def latent_attention(q_nope, q_rot, key_rows, value_rows, k_rot):
    row_count = q_nope.shape[0]
    lat_scale = (NOPE + ROPE) ** (-0.5)
    keys_float = key_rows.astype(jnp.float32)
    values_float = value_rows.astype(jnp.float32)
    krot_float = k_rot.astype(jnp.float32)

    def one_block(offset):
        q_part = lax.dynamic_slice_in_dim(q_nope, offset, QBLOCK, 0).astype(jnp.float32)
        rot_part = lax.dynamic_slice_in_dim(q_rot, offset, QBLOCK, 0).astype(jnp.float32)
        scores = (jnp.einsum('qhd,khd->hqk', q_part, keys_float) + jnp.einsum('qhr,kr->hqk', rot_part, krot_float)) * lat_scale
        row_max = lax.optimization_barrier(jnp.max(scores, axis=2, keepdims=True))
        weights = jnp.exp(scores - row_max)
        denom_sum = lax.optimization_barrier(jnp.sum(weights, axis=2))
        rounded = lax.optimization_barrier(weights.astype(jnp.bfloat16)).astype(jnp.float32)
        summed = jnp.einsum('hqk,khd->qhd', rounded, values_float)
        return (summed / denom_sum.T[:, :, None]).astype(jnp.bfloat16)
    offsets = (jnp.arange(row_count // QBLOCK) * QBLOCK).astype(jnp.int32)
    return lax.map(one_block, offsets).reshape(row_count, B_HEADS * VD)

def reference(tokens, norm_gain, window_query, window_key, window_value, sink_logit, down_query, down_latent, rotary_proj, query_gain, latent_gain, up_query, up_key, up_value, window_out, latent_out):
    row_count = tokens.shape[0]
    as_float = tokens.astype(jnp.float32)
    row_scale = lax.rsqrt(lax.optimization_barrier(jnp.mean(as_float * as_float, axis=1, keepdims=True)) + EPS)
    scaled = (as_float * norm_gain).astype(jnp.bfloat16)

    def project(weight):
        return (jnp.dot(scaled, weight, preferred_element_type=jnp.float32) * row_scale).astype(jnp.bfloat16)
    q_window = project(window_query)
    k_window = project(window_key)
    v_window = project(window_value)
    latent_q = project(down_query)
    latent_kv = project(down_latent)
    rotary_rows = project(rotary_proj)
    positions = jnp.arange(row_count, dtype=jnp.int32)
    out_window = window_attention(q_window, k_window, v_window, sink_logit)
    q_latent = jnp.dot(norm_rows(latent_q, query_gain), up_query, preferred_element_type=jnp.float32).astype(jnp.bfloat16)
    q_latent = q_latent.reshape(row_count, B_HEADS, NOPE + ROPE)
    normed_kv = norm_rows(latent_kv, latent_gain)
    key_rows = jnp.dot(normed_kv, up_key, preferred_element_type=jnp.float32).astype(jnp.bfloat16).reshape(row_count, B_HEADS, NOPE)
    value_rows = jnp.dot(normed_kv, up_value, preferred_element_type=jnp.float32).astype(jnp.bfloat16).reshape(row_count, B_HEADS, VD)
    q_nope = q_latent[..., :NOPE]
    q_rot = rotate(q_latent[..., NOPE:], positions).astype(jnp.bfloat16)
    k_rot = rotate(rotary_rows, positions).astype(jnp.bfloat16)
    out_latent = latent_attention(q_nope, q_rot, key_rows, value_rows, k_rot)
    a_share = A_HEADS * HD // N_TP
    b_share = B_HEADS * VD // N_TP
    summed = jnp.zeros((row_count, D), jnp.float32)
    for member in range(N_TP):
        head_part = jnp.dot(out_window[:, member * a_share:(member + 1) * a_share], window_out[member * a_share:(member + 1) * a_share], preferred_element_type=jnp.float32)
        head_part = head_part + jnp.dot(out_latent[:, member * b_share:(member + 1) * b_share], latent_out[member * b_share:(member + 1) * b_share], preferred_element_type=jnp.float32)
        summed = summed + lax.optimization_barrier(head_part.astype(jnp.bfloat16)).astype(jnp.float32)
    return summed.astype(jnp.bfloat16)
```

```python
import functools
import jax
import jax.numpy as jnp
from jax import lax
from jax.experimental import pallas as pl
from jax.experimental.pallas import tpu as pltpu
from jax.sharding import PartitionSpec as P

WINDOW = 128
EPS = 1e-06
THETA = 10000.0
LOG2E = 1.4426950408889634
f32, bf16 = jnp.float32, jnp.bfloat16
MESH = pl.DeviceIdType.MESH
QT = 256
NEG = -1e30


def attention_kernel(
    rows, nz, nx,
    kvm, qt, qwt, kvw, heads,
    out,
    kvb, rotx, qb, kvp, mref, lref, acc, s00, s01, s10, s11, x00, x01, x10, x11,
    osend, ssend, obuf, sbuf,
    h_send, h_recv, q_send, q_recv, qf_send, qf_recv, k_send, k_recv, kf_send, kf_recv,
    o_send, o_recv, s_send, s_recv,
):
    sp = lax.axis_index("sp")
    tp = lax.axis_index("tp")
    z, x = sp // nx, sp % nx
    nsp = nz * nx
    tiles = rows // QT
    half = kvm.shape[0] // 2

    def at(zz, xx):
        return (zz * nx + xx, tp)

    xr, xl = at(z, (x + 1) % nx), at(z, (x + nx - 1) % nx)
    zr, zl, zo = at((z + 1) % nz, x), at((z + nz - 1) % nz, x), at((z + 2) % nz, x)
    nxt, prv = ((sp + 1) % nsp, tp), ((sp + nsp - 1) % nsp, tp)

    barrier = pltpu.get_barrier_semaphore()
    for peer in (xr, xl, zr, zl, zo, nxt, prv):
        pl.semaphore_signal(barrier, inc=1, device_id=peer, device_id_type=MESH)
    pl.semaphore_wait(barrier, 7)

    def remote(src, dst, ss, rs, dev):
        return pltpu.make_async_remote_copy(
            src_ref=src, dst_ref=dst, send_sem=ss, recv_sem=rs, device_id=dev, device_id_type=MESH
        )

    halo = [
        remote(kvw.at[pl.ds(rows - WINDOW, WINDOW)], kvp.at[pl.ds(0, WINDOW)], h_send.at[0], h_recv.at[0], nxt),
        remote(kvw.at[pl.ds(0, WINDOW)], kvp.at[pl.ds(rows + WINDOW, WINDOW)], h_send.at[1], h_recv.at[1], prv),
    ]
    q_out = {}
    for order in ((0, 1), (1, 0)):
        for which, h in ((0, order[0]), (1, order[1])):
            slot, dev = ((1, zr), (2, zl))[which]
            q_out[(which, h)] = remote(
                qt.at[h], qb.at[slot, h], q_send.at[which, h], q_recv.at[which, h], dev
            )
    k_out = {}
    for order in ((0, 1), (1, 0)):
        for which, h in ((0, order[0]), (1, order[1])):
            slot, dev = ((1, xr), (2, xl))[which]
            k_out[(which, h)] = remote(
                kvm.at[pl.ds(h * half, half)], kvb.at[slot, pl.ds(h * half, half)],
                k_send.at[which, h], k_recv.at[which, h], dev,
            )
    for c in halo:
        c.start()
    for key in ((0, 0), (1, 1), (0, 1), (1, 0)):
        q_out[key].start()
        k_out[key].start()
    q_fwd = [
        remote(qb.at[1, 0], qb.at[3, 0], qf_send.at[0], qf_recv.at[0], zr),
        remote(qb.at[2, 1], qb.at[3, 1], qf_send.at[1], qf_recv.at[1], zl),
    ]
    k_fwd = [
        remote(kvb.at[1, pl.ds(0, half)], kvb.at[3, pl.ds(0, half)], kf_send.at[0], kf_recv.at[0], xr),
        remote(kvb.at[2, pl.ds(half, half)], kvb.at[3, pl.ds(half, half)], kf_send.at[1], kf_recv.at[1], xl),
    ]

    mref[...] = jnp.full(mref.shape, NEG, f32)
    lref[...] = jnp.zeros(lref.shape, f32)
    acc[...] = jnp.zeros(acc.shape, f32)
    ssend[...] = jnp.zeros(ssend.shape, f32)
    qb[0] = qt[...]
    kvb[0] = kvm[...]
    kvp[WINDOW : WINDOW + rows] = kvw[...]
    quarter = rows // 4

    def unpack(i):
        packed = kvb[i, rows : rows + quarter].astype(f32)
        for g in range(4):
            moved = packed if g == 0 else pltpu.roll(packed, 128 - 32 * g, 1)
            rotx[i, g * quarter : (g + 1) * quarter] = moved.astype(bf16)

    S = ((s00, s01), (s10, s11))
    X = ((x00, x01), (x10, x11))

    def stage_a(k, q, t, slot):
        z64, z96 = jnp.zeros((64, QT), bf16), jnp.zeros((96, QT), bf16)
        keys = jnp.concatenate([kvb[k, 0:rows], rotx[k]], axis=1)
        for h in range(2):
            qq = qb[q, h, t]
            if h == 0:
                parts = [qq[0:64], z64, qq[64:96], z96]
            else:
                parts = [z64, qq[0:64], qq[64:96], z96]
            s = jnp.dot(keys, jnp.concatenate(parts, axis=0), preferred_element_type=f32)
            S[slot][h][...] = s
            X[slot][h][...] = jnp.max(s.reshape(rows // 8, 8, QT), axis=0)

    def stage_b(k, q, t, slot):
        for h in range(2):
            old = mref[q, t, h : h + 1]
            new = jnp.maximum(old, jnp.max(X[slot][h][...], axis=0, keepdims=True))
            alpha = jnp.exp2(old - new)
            mref[q, t, h : h + 1] = new
            total = None
            for c in range(rows // 256):
                p = jnp.exp2(S[slot][h][c * 256 : (c + 1) * 256] - new).astype(bf16)
                base = rows + quarter + 256 * c + 64 * h
                v = jnp.concatenate([kvb[k, base : base + 64], kvb[k, base + 128 : base + 192]], axis=1)
                v = jnp.concatenate([v, jnp.ones((16, 256), bf16)], axis=0)
                o = jnp.dot(v, p, preferred_element_type=f32)
                total = o if total is None else total + o
            lref[q, t, h : h + 1] = lref[q, t, h : h + 1] * alpha + total[64:65]
            acc[q, t, 64 * h : 64 * h + 64] = acc[q, t, 64 * h : 64 * h + 64] * alpha + total[0:64]

    def pipeline(n, where, before=None):
        def A(i, slot):
            stage_a(*where(i), slot)

        def B(i, slot):
            stage_b(*where(i), slot)

        A(0, 0)
        loops = (n - 1) // 2

        @pl.loop(0, loops)
        def _(j):
            i = 2 * j
            if before is not None:
                before(i + 1)
            A(i + 1, 1)
            B(i, 0)
            if before is not None:
                before(i + 2)
            A(i + 2, 0)
            B(i + 1, 1)

        i = 2 * loops
        if n % 2 == 0:
            if before is not None:
                before(i + 1)
            A(i + 1, 1)
            B(i, 0)
            B(i + 1, 1)
        else:
            B(i, 0)

    def window():
        for c in halo:
            c.wait_recv()
        span = QT + 2 * WINDOW
        key_i = lax.broadcasted_iota(jnp.int32, (span, QT), 0)
        dist = key_i - WINDOW - lax.broadcasted_iota(jnp.int32, (span, QT), 1)
        dist = jnp.abs(dist)
        distf = dist.astype(f32)

        @pl.loop(0, tiles)
        def _(t):
            rows_at = pl.ds(pl.multiple_of(t * QT, QT), span)
            kv = kvp[rows_at]
            pos = sp * rows + t * QT + key_i - WINDOW
            valid = (dist <= WINDOW) & (pos >= 0) & (pos < nsp * rows)
            for h in range(2):
                slope, sink = heads[0, h], heads[1, h]
                rhs = jnp.concatenate([qwt[t, h], jnp.zeros((64, QT), bf16)], axis=0)
                s = jnp.dot(kv, rhs, preferred_element_type=f32) * 0.125
                s = jnp.where(valid, s - slope * distf, NEG)
                m = jnp.maximum(jnp.max(s, axis=0, keepdims=True), sink)
                w = jnp.exp2((s - m) * LOG2E)
                denom = jnp.sum(w, axis=0, keepdims=True) + jnp.exp2((sink - m) * LOG2E)
                w = (w * (1.0 / denom)).astype(bf16)
                o = lax.dot_general(kv, w, (((0,), (0,)), ((), ())), preferred_element_type=f32)
                S[0][0][h * 64 : h * 64 + 64] = o[64:128]
            out[pl.ds(pl.multiple_of(t * QT, QT), QT), 0:128] = S[0][0][0:128].T.astype(bf16)

    unpack(0)

    @pl.loop(0, 3)
    def _(q):
        @pl.when(q == 1)
        def _():
            window()
            for c, f in ((q_out[(0, 0)], q_fwd[0]), (q_out[(1, 1)], q_fwd[1])):
                c.wait_recv()
                f.start()
            q_out[(0, 1)].wait_recv()

        @pl.when(q == 2)
        def _():
            q_out[(1, 0)].wait_recv()
            for c, f in ((k_out[(0, 0)], k_fwd[0]), (k_out[(1, 1)], k_fwd[1])):
                c.wait_recv()
                f.start()

        pipeline(tiles, lambda i: (0, q, i))

    k_out[(0, 1)].wait_recv()
    k_out[(1, 0)].wait_recv()
    unpack(1)
    unpack(2)
    for c in q_fwd:
        c.wait_recv()

    def arrive(i):
        @pl.when(i == 3 * tiles)
        def _():
            for c in k_fwd:
                c.wait_recv()
            unpack(3)

    def finish(q):
        for t in range(tiles):
            for h in range(2):
                inv = 1.0 / lref[q, t, h : h + 1]
                osend[q, t, 64 * h : 64 * h + 64] = (acc[q, t, 64 * h : 64 * h + 64] * inv).astype(bf16)
            ssend[q, t, 0:2] = mref[q, t, 0:2]
            ssend[q, t, 2:4] = lref[q, t, 0:2]

    back = {}
    for q, slot, dev in ((3, 3, zo), (2, 1, zr), (1, 2, zl)):
        back[q] = (
            remote(osend.at[q], obuf.at[slot], o_send.at[q], o_recv.at[slot], dev),
            remote(ssend.at[q], sbuf.at[slot], s_send.at[q], s_recv.at[slot], dev),
        )

    pipeline(4 * tiles, lambda i: (i // tiles, 3, i % tiles), arrive)
    finish(3)
    for c in back[3]:
        c.start()

    @pl.loop(0, 3)
    def _(r):
        q = 2 - r
        pipeline(3 * tiles, lambda i: (1 + i // tiles, q, i % tiles))
        finish(q)
        for n in (0, 1):
            @pl.when(r == n)
            def _():
                for c in back[2 - n]:
                    c.start()

    for q in (3, 2, 1):
        for c in back[q]:
            c.wait_recv()

    @pl.loop(0, tiles)
    def _(t):
        ms = [ssend[0, t, 0:2]] + [sbuf[j, t, 0:2] for j in (1, 2, 3)]
        ls = [ssend[0, t, 2:4]] + [sbuf[j, t, 2:4] for j in (1, 2, 3)]
        top = jnp.maximum(jnp.maximum(ms[0], ms[1]), jnp.maximum(ms[2], ms[3]))
        ws = [l * jnp.exp2(m - top) for m, l in zip(ms, ls)]
        inv = 1.0 / (ws[0] + ws[1] + ws[2] + ws[3])
        for h in range(2):
            rows_h = slice(64 * h, 64 * h + 64)
            total = osend[0, t, rows_h].astype(f32) * (ws[0] * inv)[h : h + 1]
            for j in (1, 2, 3):
                total = total + obuf[j, t, rows_h].astype(f32) * (ws[j] * inv)[h : h + 1]
            S[0][0][rows_h] = total
        out[pl.ds(pl.multiple_of(t * QT, QT), QT), 128:256] = S[0][0][0:128].T.astype(bf16)

    for c in halo + list(q_out.values()) + list(k_out.values()) + q_fwd + k_fwd:
        c.wait_send()
    for q in (3, 2, 1):
        for c in back[q]:
            c.wait_send()


def attention(kvm, qt, qwt, kvw, heads, rows, nz, nx):
    tiles = rows // QT
    dma = pltpu.SemaphoreType.DMA
    V = pltpu.VMEM
    vm = pl.BlockSpec(memory_space=pltpu.VMEM)
    return pl.pallas_call(
        functools.partial(attention_kernel, rows, nz, nx),
        out_shape=jax.ShapeDtypeStruct((rows, 256), bf16),
        in_specs=[vm, vm, vm, vm, pl.BlockSpec(memory_space=pltpu.SMEM)],
        out_specs=vm,
        scratch_shapes=[
            V((4,) + kvm.shape, bf16), V((4, rows, 128), bf16), V((4, 2, tiles, 96, QT), bf16),
            V((rows + 2 * WINDOW, 128), bf16),
            V((4, tiles, 8, QT), f32), V((4, tiles, 8, QT), f32), V((4, tiles, 128, QT), f32),
        ]
        + [V((rows, QT), f32)] * 4 + [V((8, QT), f32)] * 4
        + [
            V((4, tiles, 128, QT), bf16), V((4, tiles, 8, QT), f32),
            V((4, tiles, 128, QT), bf16), V((4, tiles, 8, QT), f32),
            dma((2,)), dma((2,)), dma((2, 2)), dma((2, 2)), dma((2,)), dma((2,)),
            dma((2, 2)), dma((2, 2)), dma((2,)), dma((2,)),
            dma((4,)), dma((4,)), dma((4,)), dma((4,)),
        ],
        compiler_params=pltpu.CompilerParams(
            collective_id=1, has_side_effects=True, vmem_limit_bytes=48 * 2**20
        ),
        name="attention",
    )(kvm, qt, qwt, kvw, heads)


def rotate(vector, positions):
    half_len = vector.shape[-1] // 2
    inverse = THETA ** (-jnp.arange(half_len, dtype=f32) / half_len)
    angles = positions.astype(f32)[:, None] * inverse[None, :]
    new_shape = (angles.shape[0],) + (1,) * (vector.ndim - 2) + (half_len,)
    cosine, sine = jnp.cos(angles).reshape(new_shape), jnp.sin(angles).reshape(new_shape)
    a, b = vector[..., :half_len].astype(f32), vector[..., half_len:].astype(f32)
    return jnp.concatenate([a * cosine - b * sine, b * cosine + a * sine], axis=-1)


def norm_rows(values, gain):
    v = values.astype(f32)
    return (v * lax.rsqrt(jnp.mean(v * v, axis=1, keepdims=True) + EPS) * gain).astype(bf16)


def per_device(
    tokens, norm_gain, window_query, window_key, window_value, sink_logit, down_query, down_latent,
    rotary_proj, query_gain, latent_gain, up_query, up_key, up_value, window_out, latent_out,
):
    rows = tokens.shape[0]
    tiles = rows // QT
    width = tokens.shape[1] * lax.axis_size("tp")
    as_float = lax.all_gather(tokens, "tp", axis=1, tiled=True).astype(f32)
    scaled = (as_float * norm_gain[None, :]).astype(bf16)
    row_scale = lax.rsqrt(jnp.sum(as_float * as_float, axis=1) / width + EPS)[:, None]

    def project(weight):
        return (jnp.dot(scaled, weight, preferred_element_type=f32) * row_scale).astype(bf16)

    latent_kv, rotary_rows = project(down_latent), project(rotary_proj)
    q_window, k_window, v_window = project(window_query), project(window_key), project(window_value)
    latent_q = project(down_query)
    positions = lax.axis_index("sp") * rows + jnp.arange(rows, dtype=jnp.int32)
    k_rot = rotate(rotary_rows, positions).astype(bf16)
    normed_kv = norm_rows(latent_kv, latent_gain)
    keys = jnp.dot(normed_kv, up_key, preferred_element_type=f32).astype(bf16)
    values = jnp.dot(normed_kv, up_value, preferred_element_type=f32).astype(bf16)
    quarter = rows // 4
    rot4 = jnp.concatenate([k_rot[g * quarter : (g + 1) * quarter] for g in range(4)], axis=1)
    vt = values.reshape(rows // 128, 128, 128).transpose(0, 2, 1).reshape(rows, 128)
    kvm = jnp.concatenate([keys, rot4, vt], axis=0)
    q = jnp.dot(norm_rows(latent_q, query_gain), up_query, preferred_element_type=f32)
    q = (q * (LOG2E * 96 ** (-0.5))).reshape(rows, 2, 96)
    q = jnp.concatenate([q[..., :64], rotate(q[..., 64:], positions)], axis=-1).astype(bf16)
    qt = q.reshape(tiles, QT, 2, 96).transpose(2, 0, 3, 1)
    qwt = q_window.reshape(tiles, QT, 2, 64).transpose(0, 2, 3, 1)
    kvw = jnp.concatenate([k_window, v_window], axis=1)
    head_ids = (lax.axis_index("tp") * 2 + jnp.arange(2)).astype(f32)
    heads = jnp.stack([jnp.exp2(-8.0 * (head_ids + 1.0) / 16), sink_logit])
    nsp = lax.axis_size("sp")
    nx = 4
    mixed_in = attention(kvm, qt, qwt, kvw, heads, rows, nsp // nx, nx)
    out_rows = jnp.concatenate([window_out, latent_out], axis=0)
    part = jnp.dot(mixed_in, out_rows, preferred_element_type=f32).astype(bf16)
    return lax.psum_scatter(part, "tp", scatter_dimension=0, tiled=True)


def solution(mesh):
    col, row, rep = P(None, "tp"), P("tp", None), P()
    placed = (
        P("sp", "tp"), rep, col, col, col, P("tp"), rep, rep, rep, rep, rep, col, col, col, row, row,
    )
    return jax.shard_map(
        per_device, mesh=mesh, in_specs=placed, out_specs=P(("sp", "tp"), None), check_vma=False
    )
```

```python
import functools
import jax
import jax.numpy as jnp
import numpy as np
from jax import lax
from jax.experimental import pallas as pl
from jax.experimental.pallas import tpu as pltpu
from jax.sharding import PartitionSpec as P

D = 2048
A_HEADS = 16
WINDOW = 128
EPS = 1e-06
THETA = 10000.0
LOG2E = 1.4426950408889634
f32, bf16 = jnp.float32, jnp.bfloat16
MESH = pl.DeviceIdType.MESH
QT = 256
NEG = -1e30
NX = 4


def remote(src, dst, ss, rs, dev):
    return pltpu.make_async_remote_copy(
        src_ref=src, dst_ref=dst, send_sem=ss, recv_sem=rs, device_id=dev, device_id_type=MESH
    )


class ChipGather:
    def __init__(self, own, buf, core, right, left, partner, sems):
        ysend, yrecv, fsend, psend, precv = sems
        self.own, self.buf, self.core = own, buf, core
        self.out = {
            (s, p): remote(own[p], buf.at[s, core, p], ysend.at[s, p], yrecv.at[s, p], dev)
            for s, dev in ((1, right), (2, left))
            for p in (0, 1)
        }
        self.fwd = {
            (3, 0): remote(buf.at[1, core, 0], buf.at[3, core, 0], fsend.at[0], yrecv.at[3, 0], right),
            (3, 1): remote(buf.at[2, core, 1], buf.at[3, core, 1], fsend.at[1], yrecv.at[3, 1], left),
        }
        self.relay = {
            (s, p): remote(
                own[p] if s == 0 else buf.at[s, core, p], buf.at[s, core, p],
                psend.at[s, p], precv.at[s, p], partner,
            )
            for s in range(4)
            for p in (0, 1)
        }

    def start(self):
        for key in ((1, 0), (2, 1), (1, 1), (2, 0)):
            self.out[key].start()
        for p in (0, 1):
            self.relay[(0, p)].start()

    def arrive(self, slot, part, relay=True):
        (self.fwd if slot == 3 else self.out)[(slot, part)].wait_recv()
        if (slot, part) == (1, 0):
            self.fwd[(3, 0)].start()
        if (slot, part) == (2, 1):
            self.fwd[(3, 1)].start()
        if relay:
            self.relay[(slot, part)].start()

    def partner(self, slot, part):
        self.relay[(slot, part)].wait_recv()

    def drain(self):
        for c in list(self.out.values()) + list(self.fwd.values()) + list(self.relay.values()):
            c.wait_send()


def layer_kernel(
    rows, nz, nx, ny,
    tokens, norm_gain, query_gain, latent_gain, sinks, slopes,
    w_query, w_key, w_value, d_query, d_latent, w_rot, u_query, u_key, u_value, o_window, o_latent,
    tab_far, tab_near,
    result,
    tb, wb, wdq, wdl, wcat, wk, wv, wr, uq, uk, uv, far, near, pacc, sq,
    kvm, qwt, kvw, osw, osl, orow,
    kvb, rotx, qb, kvp, mref, lref, acc, s00, s01, s10, s11, x00, x01, x10, x11,
    osend, ssend, obuf, sbuf,
    l_sem, t_ysend, t_yrecv, t_fsend, t_psend, t_precv, w_ysend, w_yrecv, w_fsend, w_psend, w_precv,
    a_send, a_recv,
    h_send, h_recv, q_send, q_recv, qf_send, qf_recv, k_send, k_recv, kf_send, kf_recv,
    o_send, o_recv, s_send, s_recv,
):
    sp = lax.axis_index("sp")
    tp = lax.axis_index("tp")
    z, x = sp // nx, sp % nx
    y, core = tp // 2, tp % 2
    nsp, ntp = nz * nx, ny * 2
    tiles = rows // QT
    half_rows = rows // 2
    mine = rows // ntp

    loads = [
        pltpu.make_async_copy(s, d, l_sem.at[i])
        for i, (s, d) in enumerate((
            (d_query, wdq), (d_latent, wdl), (w_query, wcat.at[:, pl.ds(0, 128)]), (w_key, wk),
            (w_value, wv), (w_rot, wr), (u_query, uq), (u_key, uk), (u_value, uv),
            (tab_far.at[sp], far), (tab_near, near),
            (o_window, wb.at[0, core, 0]), (o_latent, wb.at[0, core, 1]),
        ))
    ]
    for c in loads:
        c.start()

    def at(zz, xx):
        return (zz * nx + xx, tp)

    def chip(step, cc):
        return (sp, ((y + step) % ny) * 2 + cc)

    xr, xl = at(z, (x + 1) % nx), at(z, (x + nx - 1) % nx)
    zr, zl, zo = at((z + 1) % nz, x), at((z + nz - 1) % nz, x), at((z + 2) % nz, x)
    nxt, prv = ((sp + 1) % nsp, tp), ((sp + nsp - 1) % nsp, tp)
    partner = chip(0, 1 - core)
    others = [chip(d, cc) for d in range(1, ny) for cc in (0, 1)] + [partner]

    barrier = pltpu.get_barrier_semaphore()
    peers = [xr, xl, zr, zl, zo, nxt, prv] + others
    for peer in peers:
        pl.semaphore_signal(barrier, inc=1, device_id=peer, device_id_type=MESH)
    pl.semaphore_wait(barrier, len(peers))

    tok = ChipGather(
        [tokens.at[pl.ds(p * half_rows, half_rows)] for p in (0, 1)], tb, core,
        chip(1, core), chip(ny - 1, core), partner, (t_ysend, t_yrecv, t_fsend, t_psend, t_precv),
    )
    wts = ChipGather(
        [o_window, o_latent], wb, core,
        chip(1, core), chip(ny - 1, core), partner, (w_ysend, w_yrecv, w_fsend, w_psend, w_precv),
    )
    tok.start()
    for p in (0, 1):
        tb[0, core, p] = tokens[p * half_rows : (p + 1) * half_rows]

    mref[...] = jnp.full(mref.shape, NEG, f32)
    lref[...] = jnp.zeros(lref.shape, f32)
    acc[...] = jnp.zeros(acc.shape, f32)
    ssend[...] = jnp.zeros(ssend.shape, f32)
    pacc[...] = jnp.zeros(pacc.shape, f32)
    sq[...] = jnp.zeros(sq.shape, f32)
    for c in loads:
        c.wait()
    wcat[:, 128:256] = jnp.concatenate([wk[...], wv[...]], axis=1)
    wcat[:, 256:384] = jnp.concatenate([wr[...], jnp.zeros((D, 96), bf16)], axis=1)

    @pl.loop(0, 4)
    def _(slot):
        chip_at = (y + ny - (slot + slot // 2 - 2 * (slot // 3))) % ny
        w_rows = pl.ds(pl.multiple_of(chip_at * 512, 512), 512)

        @pl.loop(0, 2)
        def _(part):
            for s in range(4):
                for p in (0, 1):
                    @pl.when((slot == s) & (part == p))
                    def _():
                        if s:
                            tok.arrive(s, p)
                        tok.partner(s, p)
                        if (s, p) == (2, 1):
                            wts.start()
            t32 = jnp.concatenate([tb[slot, 0, part], tb[slot, 1, part]], axis=1).astype(f32)
            out_rows = pl.ds(pl.multiple_of(part * half_rows, half_rows), half_rows)
            squares = t32 * t32
            sq[out_rows] += (
                squares[:, 0:128] + squares[:, 128:256] + squares[:, 256:384] + squares[:, 384:512]
            )
            scaled = (t32 * norm_gain[pl.ds(chip_at, 1), :]).astype(bf16)
            for w, lo, hi in ((wdl, 768, 1280), (wcat, 1280, 1664), (wdq, 0, 768)):
                pacc[out_rows, lo:hi] += jnp.dot(scaled, w[w_rows, :], preferred_element_type=f32)

    cos_f, sin_f = far[0:16, 0:1], far[16:32, 0:1]
    cos_n, sin_n = near[0:16, :], near[16:32, :]
    cos = cos_f * cos_n - sin_f * sin_n
    sin = sin_f * cos_n + cos_f * sin_n
    near[0:16, :] = cos
    near[16:32, :] = sin
    row_scale = lax.rsqrt(jnp.sum(sq[...], axis=1, keepdims=True) * (1.0 / D) + EPS)

    def normed(lo, hi, gain):
        v = (pacc[:, lo:hi] * row_scale).astype(bf16).astype(f32)
        scale = lax.rsqrt(jnp.sum(v * v, axis=1, keepdims=True) * (1.0 / (hi - lo)) + EPS)
        return (v * scale * gain[...]).astype(bf16)

    quarter = rows // 4
    up_kv = jnp.concatenate([uk[...], uv[...]], axis=1)
    kv = jnp.dot(normed(768, 1280, latent_gain), up_kv, preferred_element_type=f32)
    kvm[0:rows] = kv[:, 0:128].astype(bf16)
    for b in range(rows // 128):
        block = kv[128 * b : 128 * b + 128, 128:256].T
        kvm[rows + quarter + 128 * b : rows + quarter + 128 * b + 128] = block.astype(bf16)
    rr = (pacc[:, 1536:1664] * row_scale).astype(bf16).astype(f32).T
    ra, rb = rr[0:16], rr[16:32]
    cos, sin = near[0:16, :], near[16:32, :]
    turned = jnp.concatenate([ra * cos - rb * sin, rb * cos + ra * sin, jnp.zeros((96, rows), f32)], axis=0).T
    packed = turned[0:quarter]
    for g in range(1, 4):
        packed = packed + pltpu.roll(turned[g * quarter : (g + 1) * quarter], 32 * g, 1)
    kvm[rows : rows + quarter] = packed.astype(bf16)
    half = kvm.shape[0] // 2
    k_out = {}
    for order in ((0, 1), (1, 0)):
        for which, h in ((0, order[0]), (1, order[1])):
            slot, dev = ((1, xr), (2, xl))[which]
            k_out[(which, h)] = remote(
                kvm.at[pl.ds(h * half, half)], kvb.at[slot, pl.ds(h * half, half)],
                k_send.at[which, h], k_recv.at[which, h], dev,
            )
    for key in ((0, 0), (1, 1), (0, 1), (1, 0)):
        k_out[key].start()
    kvb[0] = kvm[...]

    qf = jnp.dot(normed(0, 768, query_gain), uq[...], preferred_element_type=f32) * (LOG2E * 96 ** (-0.5))
    for t in range(tiles):
        qq = jnp.concatenate([qf[QT * t : QT * t + QT], jnp.zeros((QT, 64), f32)], axis=1).T
        ct, st = cos[:, QT * t : QT * t + QT], sin[:, QT * t : QT * t + QT]
        for h in range(2):
            a, b = qq[96 * h + 64 : 96 * h + 80], qq[96 * h + 80 : 96 * h + 96]
            qb[0, h, t] = jnp.concatenate(
                [qq[96 * h : 96 * h + 64], a * ct - b * st, b * ct + a * st], axis=0
            ).astype(bf16)
    qt = qb.at[0]
    q_out = {}
    for order in ((0, 1), (1, 0)):
        for which, h in ((0, order[0]), (1, order[1])):
            slot, dev = ((1, zr), (2, zl))[which]
            q_out[(which, h)] = remote(
                qt.at[h], qb.at[slot, h], q_send.at[which, h], q_recv.at[which, h], dev
            )
    for key in ((0, 0), (1, 1), (0, 1), (1, 0)):
        q_out[key].start()

    kvw[...] = (pacc[:, 1408:1536] * row_scale).astype(bf16)
    halo = [
        remote(kvw.at[pl.ds(rows - WINDOW, WINDOW)], kvp.at[pl.ds(0, WINDOW)], h_send.at[0], h_recv.at[0], nxt),
        remote(kvw.at[pl.ds(0, WINDOW)], kvp.at[pl.ds(rows + WINDOW, WINDOW)], h_send.at[1], h_recv.at[1], prv),
    ]
    for c in halo:
        c.start()
    kvp[WINDOW : WINDOW + rows] = kvw[...]
    wq = pacc[:, 1280:1408] * row_scale
    for t in range(tiles):
        qwt[t] = wq[QT * t : QT * t + QT].T.astype(bf16).reshape(2, 64, QT)
    q_fwd = [
        remote(qb.at[1, 0], qb.at[3, 0], qf_send.at[0], qf_recv.at[0], zr),
        remote(qb.at[2, 1], qb.at[3, 1], qf_send.at[1], qf_recv.at[1], zl),
    ]
    k_fwd = [
        remote(kvb.at[1, pl.ds(0, half)], kvb.at[3, pl.ds(0, half)], kf_send.at[0], kf_recv.at[0], xr),
        remote(kvb.at[2, pl.ds(half, half)], kvb.at[3, pl.ds(half, half)], kf_send.at[1], kf_recv.at[1], xl),
    ]

    def unpack(i):
        packed = kvb[i, rows : rows + quarter].astype(f32)
        for g in range(4):
            moved = packed if g == 0 else pltpu.roll(packed, 128 - 32 * g, 1)
            rotx[i, g * quarter : (g + 1) * quarter] = moved.astype(bf16)

    def piece(part, src, d, cc):
        dev = chip(d, cc) if d else partner
        slot = (0, 1, 3, 2)[d]
        row_at = pl.ds(pl.multiple_of(dev[1] * mine, mine), mine)
        i = 2 * d + (cc if d else 0)
        return remote(
            src.at[row_at], orow.at[slot, core, part], a_send.at[part, i], a_recv.at[part, slot, core], dev
        )

    def pieces(part, src):
        keys = [(2, 0), (2, 1), (1, 0), (3, 0), (1, 1), (3, 1), (0, 0)]
        return [piece(part, src, d, cc) for d, cc in keys]

    S = ((s00, s01), (s10, s11))
    X = ((x00, x01), (x10, x11))

    def stage_a(k, q, t, slot):
        z64, z96 = jnp.zeros((64, QT), bf16), jnp.zeros((96, QT), bf16)
        keys = jnp.concatenate([kvb[k, 0:rows], rotx[k]], axis=1)
        for h in range(2):
            qq = qb[q, h, t]
            if h == 0:
                parts = [qq[0:64], z64, qq[64:96], z96]
            else:
                parts = [z64, qq[0:64], qq[64:96], z96]
            s = jnp.dot(keys, jnp.concatenate(parts, axis=0), preferred_element_type=f32)
            S[slot][h][...] = s
            X[slot][h][...] = jnp.max(s.reshape(rows // 8, 8, QT), axis=0)

    def stage_b(k, q, t, slot):
        for h in range(2):
            old = mref[q, t, h : h + 1]
            new = jnp.maximum(old, jnp.max(X[slot][h][...], axis=0, keepdims=True))
            alpha = jnp.exp2(old - new)
            mref[q, t, h : h + 1] = new
            total = None
            for c in range(rows // 256):
                p = jnp.exp2(S[slot][h][c * 256 : (c + 1) * 256] - new).astype(bf16)
                base = rows + quarter + 256 * c + 64 * h
                v = jnp.concatenate([kvb[k, base : base + 64], kvb[k, base + 128 : base + 192]], axis=1)
                v = jnp.concatenate([v, jnp.ones((16, 256), bf16)], axis=0)
                o = jnp.dot(v, p, preferred_element_type=f32)
                total = o if total is None else total + o
            lref[q, t, h : h + 1] = lref[q, t, h : h + 1] * alpha + total[64:65]
            acc[q, t, 64 * h : 64 * h + 64] = acc[q, t, 64 * h : 64 * h + 64] * alpha + total[0:64]

    def pipeline(n, where, before=None):
        def A(i, slot):
            stage_a(*where(i), slot)

        def B(i, slot):
            stage_b(*where(i), slot)

        A(0, 0)
        loops = (n - 1) // 2

        @pl.loop(0, loops)
        def _(j):
            i = 2 * j
            if before is not None:
                before(i + 1)
            A(i + 1, 1)
            B(i, 0)
            if before is not None:
                before(i + 2)
            A(i + 2, 0)
            B(i + 1, 1)

        i = 2 * loops
        if n % 2 == 0:
            if before is not None:
                before(i + 1)
            A(i + 1, 1)
            B(i, 0)
            B(i + 1, 1)
        else:
            B(i, 0)

    def window():
        for c in halo:
            c.wait_recv()
        span = QT + 2 * WINDOW
        key_i = lax.broadcasted_iota(jnp.int32, (span, QT), 0)
        dist = key_i - WINDOW - lax.broadcasted_iota(jnp.int32, (span, QT), 1)
        dist = jnp.abs(dist)
        distf = dist.astype(f32)

        @pl.loop(0, tiles)
        def _(t):
            rows_at = pl.ds(pl.multiple_of(t * QT, QT), span)
            kv = kvp[rows_at]
            pos = sp * rows + t * QT + key_i - WINDOW
            valid = (dist <= WINDOW) & (pos >= 0) & (pos < nsp * rows)
            for h in range(2):
                slope, sink = slopes[tp * 2 + h], sinks[h]
                rhs = jnp.concatenate([qwt[t, h], jnp.zeros((64, QT), bf16)], axis=0)
                s = jnp.dot(kv, rhs, preferred_element_type=f32) * 0.125
                s = jnp.where(valid, s - slope * distf, NEG)
                m = jnp.maximum(jnp.max(s, axis=0, keepdims=True), sink)
                w = jnp.exp2((s - m) * LOG2E)
                denom = jnp.sum(w, axis=0, keepdims=True) + jnp.exp2((sink - m) * LOG2E)
                w = (w * (1.0 / denom)).astype(bf16)
                o = lax.dot_general(kv, w, (((0,), (0,)), ((), ())), preferred_element_type=f32)
                S[0][0][h * 64 : h * 64 + 64] = o[64:128]
            osw[pl.ds(pl.multiple_of(t * QT, QT), QT), :] = S[0][0][0:128].T.astype(bf16)

    unpack(0)

    @pl.loop(0, 3)
    def _(q):
        @pl.when(q == 1)
        def _():
            window()
            for c in pieces(0, osw):
                c.start()
            orow[0, core, 0] = osw[pl.ds(pl.multiple_of(tp * mine, mine), mine), :]
            for c, f in ((q_out[(0, 0)], q_fwd[0]), (q_out[(1, 1)], q_fwd[1])):
                c.wait_recv()
                f.start()
            q_out[(0, 1)].wait_recv()

        @pl.when(q == 2)
        def _():
            q_out[(1, 0)].wait_recv()
            for c, f in ((k_out[(0, 0)], k_fwd[0]), (k_out[(1, 1)], k_fwd[1])):
                c.wait_recv()
                f.start()

        pipeline(tiles, lambda i: (0, q, i))

    k_out[(0, 1)].wait_recv()
    k_out[(1, 0)].wait_recv()
    unpack(1)
    unpack(2)
    for c in q_fwd:
        c.wait_recv()

    def arrive(i):
        @pl.when(i == 3 * tiles)
        def _():
            for c in k_fwd:
                c.wait_recv()
            unpack(3)

    def finish(q):
        for t in range(tiles):
            for h in range(2):
                inv = 1.0 / lref[q, t, h : h + 1]
                osend[q, t, 64 * h : 64 * h + 64] = (acc[q, t, 64 * h : 64 * h + 64] * inv).astype(bf16)
            ssend[q, t, 0:2] = mref[q, t, 0:2]
            ssend[q, t, 2:4] = lref[q, t, 0:2]

    back = {}
    for q, slot, dev in ((3, 3, zo), (2, 1, zr), (1, 2, zl)):
        back[q] = (
            remote(osend.at[q], obuf.at[slot], o_send.at[q], o_recv.at[slot], dev),
            remote(ssend.at[q], sbuf.at[slot], s_send.at[q], s_recv.at[slot], dev),
        )

    pipeline(4 * tiles, lambda i: (i // tiles, 3, i % tiles), arrive)
    finish(3)
    for c in back[3]:
        c.start()
    wts.arrive(1, 0)
    wts.arrive(2, 1)

    @pl.loop(0, 3)
    def _(r):
        q = 2 - r
        pipeline(3 * tiles, lambda i: (1 + i // tiles, q, i % tiles))
        finish(q)
        for n in (0, 1):
            @pl.when(r == n)
            def _():
                for c in back[2 - n]:
                    c.start()
                if n == 1:
                    wts.arrive(1, 1)
                    wts.arrive(2, 0)

    for q in (3, 2, 1):
        for c in back[q]:
            c.wait_recv()

    @pl.loop(0, tiles)
    def _(t):
        ms = [ssend[0, t, 0:2]] + [sbuf[j, t, 0:2] for j in (1, 2, 3)]
        ls = [ssend[0, t, 2:4]] + [sbuf[j, t, 2:4] for j in (1, 2, 3)]
        top = jnp.maximum(jnp.maximum(ms[0], ms[1]), jnp.maximum(ms[2], ms[3]))
        ws = [l * jnp.exp2(m - top) for m, l in zip(ms, ls)]
        inv = 1.0 / (ws[0] + ws[1] + ws[2] + ws[3])
        for h in range(2):
            rows_h = slice(64 * h, 64 * h + 64)
            total = osend[0, t, rows_h].astype(f32) * (ws[0] * inv)[h : h + 1]
            for j in (1, 2, 3):
                total = total + obuf[j, t, rows_h].astype(f32) * (ws[j] * inv)[h : h + 1]
            S[0][0][rows_h] = total
        osl[pl.ds(pl.multiple_of(t * QT, QT), QT), :] = S[0][0][0:128].T.astype(bf16)

    for c in pieces(1, osl):
        c.start()
    orow[0, core, 1] = osl[pl.ds(pl.multiple_of(tp * mine, mine), mine), :]
    wts.arrive(3, 0)
    wts.arrive(3, 1)
    for s in range(4):
        for p in (0, 1):
            wts.partner(s, p)
            for cc in (0, 1) if s else (1 - core,):
                there = orow.at[s, cc, p]
                remote(there, there, a_send.at[p, 0], a_recv.at[p, s, cc], partner).wait_recv()

    @pl.loop(0, D // 512)
    def _(b):
        cols = pl.ds(pl.multiple_of(b * 512, 512), 512)
        total = None
        for s in range(4):
            for cc in (0, 1):
                o = jnp.concatenate([orow[s, cc, 0], orow[s, cc, 1]], axis=1)
                w = jnp.concatenate([wb[s, cc, 0, :, cols], wb[s, cc, 1, :, cols]], axis=0)
                g = jnp.dot(o, w, preferred_element_type=f32).astype(bf16).astype(f32)
                total = g if total is None else total + g
        result[:, cols] = total.astype(bf16)

    for c in halo + list(q_out.values()) + list(k_out.values()) + q_fwd + k_fwd:
        c.wait_send()
    for q in (3, 2, 1):
        for c in back[q]:
            c.wait_send()
    for part, src in ((0, osw), (1, osl)):
        for c in pieces(part, src):
            c.wait_send()
    tok.drain()
    wts.drain()


def angle_tables(rows, nsp):
    inverse = THETA ** (-np.arange(16, dtype=np.float64) / 16)
    far = np.arange(nsp)[:, None] * rows * inverse[None, :]
    far = np.concatenate([np.cos(far), np.sin(far)], axis=1)[:, :, None]
    near = inverse[:, None] * np.arange(rows)[None, :]
    near = np.concatenate([np.cos(near), np.sin(near)], axis=0)
    return np.broadcast_to(far, (nsp, 32, 128)).astype(np.float32), near.astype(np.float32)


def per_device(
    nsp, ntp, tokens, norm_gain, window_query, window_key, window_value, sink_logit, down_query,
    down_latent, rotary_proj, query_gain, latent_gain, up_query, up_key, up_value, window_out, latent_out,
):
    rows = tokens.shape[0]
    tiles, mine, half_rows = rows // QT, rows // ntp, rows // 2
    far, near = angle_tables(rows, nsp)
    slopes = np.exp2(-8.0 * (np.arange(A_HEADS) + 1.0) / A_HEADS).astype(np.float32)
    dma, V = pltpu.SemaphoreType.DMA, pltpu.VMEM
    vm, smem = pl.BlockSpec(memory_space=pltpu.VMEM), pl.BlockSpec(memory_space=pltpu.SMEM)
    hbm = pl.BlockSpec(memory_space=pl.ANY)
    gather_sems = [dma((3, 2)), dma((4, 2)), dma((2,)), dma((4, 2)), dma((4, 2))]
    message = rows + rows // 4 + rows
    return pl.pallas_call(
        functools.partial(layer_kernel, rows, nsp // NX, NX, ntp // 2),
        out_shape=jax.ShapeDtypeStruct((mine, D), bf16),
        in_specs=[vm, vm, vm, vm, smem, smem] + [hbm] * 13,
        out_specs=vm,
        scratch_shapes=[
            V((4, 2, 2, half_rows, 256), bf16), V((4, 2, 2, 128, D), bf16),
            V((D, 768), bf16), V((D, 512), bf16), V((D, 384), bf16),
            V((D, 64), bf16), V((D, 64), bf16), V((D, 32), bf16),
            V((768, 192), bf16), V((512, 128), bf16), V((512, 128), bf16),
            V((32, 128), f32), V((32, rows), f32), V((rows, 1664), f32), V((rows, 128), f32),
            V((message, 128), bf16), V((tiles, 2, 64, QT), bf16), V((rows, 128), bf16),
            V((rows, 128), bf16), V((rows, 128), bf16), V((4, 2, 2, mine, 128), bf16),
            V((4, message, 128), bf16), V((4, rows, 128), bf16), V((4, 2, tiles, 96, QT), bf16),
            V((rows + 2 * WINDOW, 128), bf16),
            V((4, tiles, 8, QT), f32), V((4, tiles, 8, QT), f32), V((4, tiles, 128, QT), f32),
        ]
        + [V((rows, QT), f32)] * 4 + [V((8, QT), f32)] * 4
        + [
            V((4, tiles, 128, QT), bf16), V((4, tiles, 8, QT), f32),
            V((4, tiles, 128, QT), bf16), V((4, tiles, 8, QT), f32),
            dma((13,)),
        ]
        + gather_sems + gather_sems
        + [
            dma((2, 8)), dma((2, 4, 2)),
            dma((2,)), dma((2,)), dma((2, 2)), dma((2, 2)), dma((2,)), dma((2,)),
            dma((2, 2)), dma((2, 2)), dma((2,)), dma((2,)),
            dma((4,)), dma((4,)), dma((4,)), dma((4,)),
        ],
        compiler_params=pltpu.CompilerParams(
            collective_id=1, has_side_effects=True, vmem_limit_bytes=60 * 2**20
        ),
        name="layer",
    )(
        tokens, norm_gain.reshape(4, D // 4), query_gain.reshape(1, -1), latent_gain.reshape(1, -1),
        sink_logit, jnp.asarray(slopes), window_query, window_key, window_value, down_query, down_latent,
        rotary_proj, up_query, up_key, up_value, window_out, latent_out, jnp.asarray(far), jnp.asarray(near),
    )


def solution(mesh):
    col, row, rep = P(None, "tp"), P("tp", None), P()
    placed = (
        P("sp", "tp"), rep, col, col, col, P("tp"), rep, rep, rep, rep, rep, col, col, col, row, row,
    )
    body = functools.partial(per_device, mesh.shape["sp"], mesh.shape["tp"])
    return jax.shard_map(
        body, mesh=mesh, in_specs=placed, out_specs=P(("sp", "tp"), None), check_vma=False
    )
```

```python
import functools
import jax
import jax.numpy as jnp
import numpy as np
from jax import lax
from jax.experimental import pallas as pl
from jax.experimental.pallas import tpu as pltpu
from jax.sharding import PartitionSpec as P

D = 2048
A_HEADS = 16
WINDOW = 128
EPS = 1e-06
THETA = 10000.0
LOG2E = 1.4426950408889634
f32, bf16 = jnp.float32, jnp.bfloat16
MESH = pl.DeviceIdType.MESH
QT = 256
NEG = -1e30
NX = 4


def remote(src, dst, ss, rs, dev):
    return pltpu.make_async_remote_copy(
        src_ref=src, dst_ref=dst, send_sem=ss, recv_sem=rs, device_id=dev, device_id_type=MESH
    )


class ChipGather:
    def __init__(self, own, buf, core, right, left, partner, sems):
        ysend, yrecv, fsend, psend, precv = sems
        self.own, self.buf, self.core = own, buf, core
        self.out = {
            (s, p): remote(own[p], buf.at[s, core, p], ysend.at[s, p], yrecv.at[s, p], dev)
            for s, dev in ((1, right), (2, left))
            for p in (0, 1)
        }
        self.fwd = {
            (3, 0): remote(buf.at[1, core, 0], buf.at[3, core, 0], fsend.at[0], yrecv.at[3, 0], right),
            (3, 1): remote(buf.at[2, core, 1], buf.at[3, core, 1], fsend.at[1], yrecv.at[3, 1], left),
        }
        self.relay = {
            (s, p): remote(
                own[p] if s == 0 else buf.at[s, core, p], buf.at[s, core, p],
                psend.at[s, p], precv.at[s, p], partner,
            )
            for s in range(4)
            for p in (0, 1)
        }

    def start(self):
        for key in ((1, 0), (2, 1), (1, 1), (2, 0)):
            self.out[key].start()
        for p in (0, 1):
            self.relay[(0, p)].start()

    def arrive(self, slot, part, relay=True):
        (self.fwd if slot == 3 else self.out)[(slot, part)].wait_recv()
        if (slot, part) == (1, 0):
            self.fwd[(3, 0)].start()
        if (slot, part) == (2, 1):
            self.fwd[(3, 1)].start()
        if relay:
            self.relay[(slot, part)].start()

    def partner(self, slot, part):
        self.relay[(slot, part)].wait_recv()

    def drain(self):
        for c in list(self.out.values()) + list(self.fwd.values()) + list(self.relay.values()):
            c.wait_send()


def layer_kernel(
    rows, nz, nx, ny,
    tokens, norm_gain, query_gain, latent_gain, sinks, slopes,
    w_query, w_key, w_value, d_query, d_latent, w_rot, u_query, u_key, u_value, o_window, o_latent,
    tab_far, tab_near,
    result,
    tb, wb, wdq, wdl, wcat, wnarrow, uq, uk, uv, far, near, pacc, sq,
    kvm, qwt, kvw, osw, osl, orow,
    kvb, rotx, qb, kvp, mref, lref, acc, s00, s01, s10, s11, x00, x01, x10, x11,
    osend, ssend, obuf, sbuf,
    l_sem, t_ysend, t_yrecv, t_fsend, t_psend, t_precv, w_ysend, w_yrecv, w_fsend, w_psend, w_precv,
    a_send, a_recv,
    h_send, h_recv, q_send, q_recv, qf_send, qf_recv, k_send, k_recv, kf_send, kf_recv,
    o_send, o_recv, s_send, s_recv,
):
    sp = lax.axis_index("sp")
    tp = lax.axis_index("tp")
    z, x = sp // nx, sp % nx
    y, core = tp // 2, tp % 2
    nsp, ntp = nz * nx, ny * 2
    tiles = rows // QT
    half_rows = rows // 2
    mine = rows // ntp

    loads = [
        pltpu.make_async_copy(s, d, l_sem.at[i])
        for i, (s, d) in enumerate((
            (d_query, wdq), (d_latent, wdl), (w_query, wcat.at[:, pl.ds(0, 128)]),
            (w_key, wnarrow.at[pl.ds(0, 64)]), (w_value, wnarrow.at[pl.ds(64, 64)]),
            (w_rot, wnarrow.at[pl.ds(128, 32)]), (u_query, uq), (u_key, uk), (u_value, uv),
            (tab_far.at[sp], far), (tab_near, near),
            (o_window, wb.at[0, core, 0]), (o_latent, wb.at[0, core, 1]),
        ))
    ]
    for c in loads:
        c.start()

    def at(zz, xx):
        return (zz * nx + xx, tp)

    def chip(step, cc):
        return (sp, ((y + step) % ny) * 2 + cc)

    xr, xl = at(z, (x + 1) % nx), at(z, (x + nx - 1) % nx)
    zr, zl, zo = at((z + 1) % nz, x), at((z + nz - 1) % nz, x), at((z + 2) % nz, x)
    nxt, prv = ((sp + 1) % nsp, tp), ((sp + nsp - 1) % nsp, tp)
    partner = chip(0, 1 - core)
    others = [chip(d, cc) for d in range(1, ny) for cc in (0, 1)] + [partner]

    barrier = pltpu.get_barrier_semaphore()
    peers = [xr, xl, zr, zl, zo, nxt, prv] + others
    for peer in peers:
        pl.semaphore_signal(barrier, inc=1, device_id=peer, device_id_type=MESH)
    pl.semaphore_wait(barrier, len(peers))

    tok = ChipGather(
        [tokens.at[pl.ds(p * half_rows, half_rows)] for p in (0, 1)], tb, core,
        chip(1, core), chip(ny - 1, core), partner, (t_ysend, t_yrecv, t_fsend, t_psend, t_precv),
    )
    wts = ChipGather(
        [o_window, o_latent], wb, core,
        chip(1, core), chip(ny - 1, core), partner, (w_ysend, w_yrecv, w_fsend, w_psend, w_precv),
    )
    tok.start()
    for p in (0, 1):
        tb[0, core, p] = tokens[p * half_rows : (p + 1) * half_rows]

    mref[...] = jnp.full(mref.shape, NEG, f32)
    lref[...] = jnp.zeros(lref.shape, f32)
    acc[...] = jnp.zeros(acc.shape, f32)
    ssend[...] = jnp.zeros(ssend.shape, f32)
    pacc[...] = jnp.zeros(pacc.shape, f32)
    sq[...] = jnp.zeros(sq.shape, f32)
    wnarrow[160:256] = jnp.zeros((96, D), bf16)
    for c in loads:
        c.wait()

    @pl.loop(0, D // 128)
    def _(b):
        at_b = pl.ds(pl.multiple_of(b * 128, 128), 128)
        wcat[at_b, 128:384] = wnarrow[:, at_b].astype(f32).T.astype(bf16)

    arrivals = {(1, 0): ((1, 0), (2, 1)), (1, 1): ((1, 1), (2, 0)), (3, 0): ((3, 0), (3, 1))}

    @pl.loop(0, 4)
    def _(slot):
        chip_at = (y + ny - (slot + slot // 2 - 2 * (slot // 3))) % ny
        w_rows = pl.ds(pl.multiple_of(chip_at * 512, 512), 512)

        @pl.loop(0, 2)
        def _(part):
            for s in range(4):
                for p in (0, 1):
                    @pl.when((slot == s) & (part == p))
                    def _():
                        for key in arrivals.get((s, p), ()):
                            tok.arrive(*key)
                        tok.partner(s, p)
            t32 = jnp.concatenate([tb[slot, 0, part], tb[slot, 1, part]], axis=1).astype(f32)
            out_rows = pl.ds(pl.multiple_of(part * half_rows, half_rows), half_rows)
            squares = t32 * t32
            sq[out_rows] += (
                squares[:, 0:128] + squares[:, 128:256] + squares[:, 256:384] + squares[:, 384:512]
            )
            scaled = (t32 * norm_gain[:, w_rows]).astype(bf16)
            for w, lo, hi in ((wdl, 768, 1280), (wcat, 1280, 1664), (wdq, 0, 768)):
                pacc[out_rows, lo:hi] += jnp.dot(scaled, w[w_rows, :], preferred_element_type=f32)

    cos_f, sin_f = far[0:16, 0:1], far[16:32, 0:1]
    cos_n, sin_n = near[0:16, :], near[16:32, :]
    cos = cos_f * cos_n - sin_f * sin_n
    sin = sin_f * cos_n + cos_f * sin_n
    near[0:16, :] = cos
    near[16:32, :] = sin
    row_scale = lax.rsqrt(jnp.sum(sq[...], axis=1, keepdims=True) * (1.0 / D) + EPS)

    def normed(lo, hi, gain):
        v = (pacc[:, lo:hi] * row_scale).astype(bf16).astype(f32)
        scale = lax.rsqrt(jnp.sum(v * v, axis=1, keepdims=True) * (1.0 / (hi - lo)) + EPS)
        return (v * scale * gain).astype(bf16)

    kvw[...] = (pacc[:, 1408:1536] * row_scale).astype(bf16)
    halo = [
        remote(kvw.at[pl.ds(rows - WINDOW, WINDOW)], kvp.at[pl.ds(0, WINDOW)], h_send.at[0], h_recv.at[0], nxt),
        remote(kvw.at[pl.ds(0, WINDOW)], kvp.at[pl.ds(rows + WINDOW, WINDOW)], h_send.at[1], h_recv.at[1], prv),
    ]
    for c in halo:
        c.start()
    quarter = rows // 4
    up_kv = jnp.concatenate([uk[...], uv[...]], axis=1)
    kv = jnp.dot(normed(768, 1280, latent_gain[...]), up_kv, preferred_element_type=f32)
    kvm[0:rows] = kv[:, 0:128].astype(bf16)
    for b in range(rows // 128):
        block = kv[128 * b : 128 * b + 128, 128:256].T
        kvm[rows + quarter + 128 * b : rows + quarter + 128 * b + 128] = block.astype(bf16)
    rr = (pacc[:, 1536:1664] * row_scale).astype(bf16).astype(f32).T
    ra, rb = rr[0:16], rr[16:32]
    cos, sin = near[0:16, :], near[16:32, :]
    turned = jnp.concatenate([ra * cos - rb * sin, rb * cos + ra * sin, jnp.zeros((96, rows), f32)], axis=0).T
    packed = turned[0:quarter]
    for g in range(1, 4):
        packed = packed + pltpu.roll(turned[g * quarter : (g + 1) * quarter], 32 * g, 1)
    kvm[rows : rows + quarter] = packed.astype(bf16)
    half = kvm.shape[0] // 2
    k_out = {}
    for order in ((0, 1), (1, 0)):
        for which, h in ((0, order[0]), (1, order[1])):
            slot, dev = ((1, xr), (2, xl))[which]
            k_out[(which, h)] = remote(
                kvm.at[pl.ds(h * half, half)], kvb.at[slot, pl.ds(h * half, half)],
                k_send.at[which, h], k_recv.at[which, h], dev,
            )
    for key in ((0, 0), (1, 1), (0, 1), (1, 0)):
        k_out[key].start()
    kvb[0] = kvm[...]

    qf = lax.dot_general(
        uq[...], normed(0, 768, jnp.concatenate([query_gain[i : i + 1] for i in range(6)], axis=1)), (((1,), (1,)), ((), ())), preferred_element_type=f32
    ) * (LOG2E * 96 ** (-0.5))
    for h in range(2):
        a, b = qf[96 * h + 64 : 96 * h + 80], qf[96 * h + 80 : 96 * h + 96]
        whole = jnp.concatenate(
            [qf[96 * h : 96 * h + 64], a * cos - b * sin, b * cos + a * sin], axis=0
        ).astype(bf16)
        for t in range(tiles):
            qb[0, h, t] = whole[:, QT * t : QT * t + QT]
    qt = qb.at[0]
    q_out = {}
    for order in ((0, 1), (1, 0)):
        for which, h in ((0, order[0]), (1, order[1])):
            slot, dev = ((1, zr), (2, zl))[which]
            q_out[(which, h)] = remote(
                qt.at[h], qb.at[slot, h], q_send.at[which, h], q_recv.at[which, h], dev
            )
    for key in ((0, 0), (1, 1), (0, 1), (1, 0)):
        q_out[key].start()

    wts.start()
    kvp[WINDOW : WINDOW + rows] = kvw[...]
    wq = pacc[:, 1280:1408] * row_scale
    for t in range(tiles):
        qwt[t] = wq[QT * t : QT * t + QT].T.astype(bf16).reshape(2, 64, QT)
    q_fwd = [
        remote(qb.at[1, 0], qb.at[3, 0], qf_send.at[0], qf_recv.at[0], zr),
        remote(qb.at[2, 1], qb.at[3, 1], qf_send.at[1], qf_recv.at[1], zl),
    ]
    k_fwd = [
        remote(kvb.at[1, pl.ds(0, half)], kvb.at[3, pl.ds(0, half)], kf_send.at[0], kf_recv.at[0], xr),
        remote(kvb.at[2, pl.ds(half, half)], kvb.at[3, pl.ds(half, half)], kf_send.at[1], kf_recv.at[1], xl),
    ]

    def unpack(i):
        packed = kvb[i, rows : rows + quarter].astype(f32)
        for g in range(4):
            moved = packed if g == 0 else pltpu.roll(packed, 128 - 32 * g, 1)
            rotx[i, g * quarter : (g + 1) * quarter] = moved.astype(bf16)

    def piece(part, src, d, cc):
        dev = chip(d, cc) if d else partner
        slot = (0, 1, 3, 2)[d]
        row_at = pl.ds(pl.multiple_of(dev[1] * mine, mine), mine)
        i = 2 * d + (cc if d else 0)
        return remote(
            src.at[row_at], orow.at[slot, core, part], a_send.at[part, i], a_recv.at[part, slot, core], dev
        )

    def pieces(part, src):
        keys = [(2, 0), (2, 1), (1, 0), (3, 0), (1, 1), (3, 1), (0, 0)]
        return [piece(part, src, d, cc) for d, cc in keys]

    S = ((s00, s01), (s10, s11))
    X = ((x00, x01), (x10, x11))

    def stage_a(k, q, t, slot):
        z64, z96 = jnp.zeros((64, QT), bf16), jnp.zeros((96, QT), bf16)
        keys = jnp.concatenate([kvb[k, 0:rows], rotx[k]], axis=1)
        for h in range(2):
            qq = qb[q, h, t]
            if h == 0:
                parts = [qq[0:64], z64, qq[64:96], z96]
            else:
                parts = [z64, qq[0:64], qq[64:96], z96]
            s = jnp.dot(keys, jnp.concatenate(parts, axis=0), preferred_element_type=f32)
            S[slot][h][...] = s
            X[slot][h][...] = jnp.max(s.reshape(rows // 8, 8, QT), axis=0)

    def stage_b(k, q, t, slot):
        for h in range(2):
            old = mref[q, t, h : h + 1]
            new = jnp.maximum(old, jnp.max(X[slot][h][...], axis=0, keepdims=True))
            alpha = jnp.exp2(old - new)
            mref[q, t, h : h + 1] = new
            total = None
            for c in range(rows // 256):
                p = jnp.exp2(S[slot][h][c * 256 : (c + 1) * 256] - new).astype(bf16)
                base = rows + quarter + 256 * c + 64 * h
                v = jnp.concatenate([kvb[k, base : base + 64], kvb[k, base + 128 : base + 192]], axis=1)
                v = jnp.concatenate([v, jnp.ones((16, 256), bf16)], axis=0)
                o = jnp.dot(v, p, preferred_element_type=f32)
                total = o if total is None else total + o
            lref[q, t, h : h + 1] = lref[q, t, h : h + 1] * alpha + total[64:65]
            acc[q, t, 64 * h : 64 * h + 64] = acc[q, t, 64 * h : 64 * h + 64] * alpha + total[0:64]

    def pipeline(n, where, before=None, after=None):
        def A(i, slot):
            stage_a(*where(i), slot)

        def B(i, slot):
            stage_b(*where(i), slot)
            if after is not None:
                after(i)

        A(0, 0)
        loops = (n - 1) // 2

        @pl.loop(0, loops)
        def _(j):
            i = 2 * j
            if before is not None:
                before(i + 1)
            A(i + 1, 1)
            B(i, 0)
            if before is not None:
                before(i + 2)
            A(i + 2, 0)
            B(i + 1, 1)

        i = 2 * loops
        if n % 2 == 0:
            if before is not None:
                before(i + 1)
            A(i + 1, 1)
            B(i, 0)
            B(i + 1, 1)
        else:
            B(i, 0)

    def window():
        for c in halo:
            c.wait_recv()
        span = QT + 2 * WINDOW
        key_i = lax.broadcasted_iota(jnp.int32, (span, QT), 0)
        dist = key_i - WINDOW - lax.broadcasted_iota(jnp.int32, (span, QT), 1)
        dist = jnp.abs(dist)
        distf = dist.astype(f32)

        @pl.loop(0, tiles)
        def _(t):
            rows_at = pl.ds(pl.multiple_of(t * QT, QT), span)
            kv = kvp[rows_at]
            pos = sp * rows + t * QT + key_i - WINDOW
            valid = (dist <= WINDOW) & (pos >= 0) & (pos < nsp * rows)
            for h in range(2):
                slope, sink = slopes[tp * 2 + h], sinks[h]
                rhs = jnp.concatenate([qwt[t, h], jnp.zeros((64, QT), bf16)], axis=0)
                s = jnp.dot(kv, rhs, preferred_element_type=f32) * 0.125
                s = jnp.where(valid, s - slope * distf, NEG)
                m = jnp.maximum(jnp.max(s, axis=0, keepdims=True), sink)
                w = jnp.exp2((s - m) * LOG2E)
                denom = jnp.sum(w, axis=0, keepdims=True) + jnp.exp2((sink - m) * LOG2E)
                w = (w * (1.0 / denom)).astype(bf16)
                o = lax.dot_general(kv, w, (((0,), (0,)), ((), ())), preferred_element_type=f32)
                S[0][0][h * 64 : h * 64 + 64] = o[64:128]
            osw[pl.ds(pl.multiple_of(t * QT, QT), QT), :] = S[0][0][0:128].T.astype(bf16)

    unpack(0)

    @pl.loop(0, 3)
    def _(q):
        @pl.when(q == 1)
        def _():
            window()
            for c in pieces(0, osw):
                c.start()
            orow[0, core, 0] = osw[pl.ds(pl.multiple_of(tp * mine, mine), mine), :]
            for c, f in ((q_out[(0, 0)], q_fwd[0]), (q_out[(1, 1)], q_fwd[1])):
                c.wait_recv()
                f.start()
            q_out[(0, 1)].wait_recv()

        @pl.when(q == 2)
        def _():
            q_out[(1, 0)].wait_recv()
            for c, f in ((k_out[(0, 0)], k_fwd[0]), (k_out[(1, 1)], k_fwd[1])):
                c.wait_recv()
                f.start()

        pipeline(tiles, lambda i: (0, q, i))

    k_out[(0, 1)].wait_recv()
    k_out[(1, 0)].wait_recv()
    unpack(1)
    unpack(2)
    for c in q_fwd:
        c.wait_recv()

    def arrive(i):
        @pl.when(i == 3 * tiles)
        def _():
            for c in k_fwd:
                c.wait_recv()
            unpack(3)

    def finish(q, t):
        for h in range(2):
            inv = 1.0 / lref[q, t, h : h + 1]
            osend[q, t, 64 * h : 64 * h + 64] = (acc[q, t, 64 * h : 64 * h + 64] * inv).astype(bf16)
        ssend[q, t, 0:2] = mref[q, t, 0:2]
        ssend[q, t, 2:4] = lref[q, t, 0:2]

    def back(q, t):
        slot, dev = {3: (3, zo), 2: (1, zr), 1: (2, zl)}[q]
        return (
            remote(osend.at[q, t], obuf.at[slot, t], o_send.at[q, t], o_recv.at[slot, t], dev),
            remote(ssend.at[q, t], sbuf.at[slot, t], s_send.at[q, t], s_recv.at[slot, t], dev),
        )

    pipeline(4 * tiles, lambda i: (i // tiles, 3, i % tiles), arrive)
    for t in range(tiles):
        finish(3, t)
    for t in range(tiles):
        for c in back(3, t):
            c.start()
    wts.arrive(1, 0)
    wts.arrive(2, 1)

    @pl.loop(0, 3)
    def _(r):
        q = 2 - r

        def done(i):
            @pl.when(i % 3 == 2)
            def _():
                finish(q, i // 3)
                for n in (0, 1):
                    @pl.when(r == n)
                    def _():
                        for c in back(2 - n, i // 3):
                            c.start()

        pipeline(3 * tiles, lambda i: (1 + i % 3, q, i // 3), after=done)

        @pl.when(r == 1)
        def _():
            wts.arrive(1, 1)
            wts.arrive(2, 0)

    for q in (3, 2, 1):
        for t in range(tiles):
            for c in back(q, t):
                c.wait_recv()

    @pl.loop(0, tiles)
    def _(t):
        ms = [ssend[0, t, 0:2]] + [sbuf[j, t, 0:2] for j in (1, 2, 3)]
        ls = [ssend[0, t, 2:4]] + [sbuf[j, t, 2:4] for j in (1, 2, 3)]
        top = jnp.maximum(jnp.maximum(ms[0], ms[1]), jnp.maximum(ms[2], ms[3]))
        ws = [l * jnp.exp2(m - top) for m, l in zip(ms, ls)]
        inv = 1.0 / (ws[0] + ws[1] + ws[2] + ws[3])
        for h in range(2):
            rows_h = slice(64 * h, 64 * h + 64)
            total = osend[0, t, rows_h].astype(f32) * (ws[0] * inv)[h : h + 1]
            for j in (1, 2, 3):
                total = total + obuf[j, t, rows_h].astype(f32) * (ws[j] * inv)[h : h + 1]
            S[0][0][rows_h] = total
        osl[pl.ds(pl.multiple_of(t * QT, QT), QT), :] = S[0][0][0:128].T.astype(bf16)

    for c in pieces(1, osl):
        c.start()
    orow[0, core, 1] = osl[pl.ds(pl.multiple_of(tp * mine, mine), mine), :]
    wts.arrive(3, 0)
    wts.arrive(3, 1)
    for s in range(4):
        for p in (0, 1):
            wts.partner(s, p)
            for cc in (0, 1) if s else (1 - core,):
                there = orow.at[s, cc, p]
                remote(there, there, a_send.at[p, 0], a_recv.at[p, s, cc], partner).wait_recv()

    @pl.loop(0, D // 512)
    def _(b):
        cols = pl.ds(pl.multiple_of(b * 512, 512), 512)
        total = None
        for s in range(4):
            for cc in (0, 1):
                o = jnp.concatenate([orow[s, cc, 0], orow[s, cc, 1]], axis=1)
                w = jnp.concatenate([wb[s, cc, 0, :, cols], wb[s, cc, 1, :, cols]], axis=0)
                g = jnp.dot(o, w, preferred_element_type=f32).astype(bf16).astype(f32)
                total = g if total is None else total + g
        result[:, cols] = total.astype(bf16)

    for c in halo + list(q_out.values()) + list(k_out.values()) + q_fwd + k_fwd:
        c.wait_send()
    for q in (3, 2, 1):
        for t in range(tiles):
            for c in back(q, t):
                c.wait_send()
    for part, src in ((0, osw), (1, osl)):
        for c in pieces(part, src):
            c.wait_send()
    tok.drain()
    wts.drain()


def angle_tables(rows, nsp):
    inverse = THETA ** (-np.arange(16, dtype=np.float64) / 16)
    far = np.arange(nsp)[:, None] * rows * inverse[None, :]
    far = np.concatenate([np.cos(far), np.sin(far)], axis=1)[:, :, None]
    near = inverse[:, None] * np.arange(rows)[None, :]
    near = np.concatenate([np.cos(near), np.sin(near)], axis=0)
    return np.broadcast_to(far, (nsp, 32, 128)).astype(np.float32), near.astype(np.float32)


def per_device(
    nsp, ntp, tokens, norm_gain, window_query, window_key, window_value, sink_logit, down_query,
    down_latent, rotary_proj, query_gain, latent_gain, up_query, up_key, up_value, window_out, latent_out,
):
    rows = tokens.shape[0]
    tiles, mine, half_rows = rows // QT, rows // ntp, rows // 2
    far, near = angle_tables(rows, nsp)
    slopes = np.exp2(-8.0 * (np.arange(A_HEADS) + 1.0) / A_HEADS).astype(np.float32)
    dma, V = pltpu.SemaphoreType.DMA, pltpu.VMEM
    vm, smem = pl.BlockSpec(memory_space=pltpu.VMEM), pl.BlockSpec(memory_space=pltpu.SMEM)
    hbm = pl.BlockSpec(memory_space=pl.ANY)
    gather_sems = [dma((3, 2)), dma((4, 2)), dma((2,)), dma((4, 2)), dma((4, 2))]
    message = rows + rows // 4 + rows
    return pl.pallas_call(
        functools.partial(layer_kernel, rows, nsp // NX, NX, ntp // 2),
        out_shape=jax.ShapeDtypeStruct((mine, D), bf16),
        in_specs=[vm, vm, vm, vm, smem, smem] + [hbm] * 13,
        out_specs=vm,
        scratch_shapes=[
            V((4, 2, 2, half_rows, 256), bf16), V((4, 2, 2, 128, D), bf16),
            V((D, 768), bf16), V((D, 512), bf16), V((D, 384), bf16),
            V((256, D), bf16),
            V((192, 768), bf16), V((512, 128), bf16), V((512, 128), bf16),
            V((32, 128), f32), V((32, rows), f32), V((rows, 1664), f32), V((rows, 128), f32),
            V((message, 128), bf16), V((tiles, 2, 64, QT), bf16), V((rows, 128), bf16),
            V((rows, 128), bf16), V((rows, 128), bf16), V((4, 2, 2, mine, 128), bf16),
            V((4, message, 128), bf16), V((4, rows, 128), bf16), V((4, 2, tiles, 96, QT), bf16),
            V((rows + 2 * WINDOW, 128), bf16),
            V((4, tiles, 8, QT), f32), V((4, tiles, 8, QT), f32), V((4, tiles, 128, QT), f32),
        ]
        + [V((rows, QT), f32)] * 4 + [V((8, QT), f32)] * 4
        + [
            V((4, tiles, 128, QT), bf16), V((4, tiles, 8, QT), f32),
            V((4, tiles, 128, QT), bf16), V((4, tiles, 8, QT), f32),
            dma((13,)),
        ]
        + gather_sems + gather_sems
        + [
            dma((2, 8)), dma((2, 4, 2)),
            dma((2,)), dma((2,)), dma((2, 2)), dma((2, 2)), dma((2,)), dma((2,)),
            dma((2, 2)), dma((2, 2)), dma((2,)), dma((2,)),
            dma((4, tiles)), dma((4, tiles)), dma((4, tiles)), dma((4, tiles)),
        ],
        compiler_params=pltpu.CompilerParams(
            collective_id=1, has_side_effects=True, vmem_limit_bytes=60 * 2**20
        ),
        name="layer",
    )(
        tokens, norm_gain.reshape(1, D), query_gain.reshape(6, 128), latent_gain.reshape(1, -1),
        sink_logit, jnp.asarray(slopes), window_query, window_key.T, window_value.T, down_query, down_latent,
        rotary_proj.T, up_query.T, up_key, up_value, window_out, latent_out, jnp.asarray(far), jnp.asarray(near),
    )


def solution(mesh):
    col, row, rep = P(None, "tp"), P("tp", None), P()
    placed = (
        P("sp", "tp"), rep, col, col, col, P("tp"), rep, rep, rep, rep, rep, col, col, col, row, row,
    )
    body = functools.partial(per_device, mesh.shape["sp"], mesh.shape["tp"])
    return jax.shard_map(
        body, mesh=mesh, in_specs=placed, out_specs=P(("sp", "tp"), None), check_vma=False
    )
```

```python
import functools
import jax
import jax.numpy as jnp
import numpy as np
from jax import lax
from jax.experimental import pallas as pl
from jax.experimental.pallas import tpu as pltpu
from jax.sharding import PartitionSpec as P

D = 2048
A_HEADS = 16
WINDOW = 128
EPS = 1e-06
THETA = 10000.0
LOG2E = 1.4426950408889634
f32, bf16 = jnp.float32, jnp.bfloat16
MESH = pl.DeviceIdType.MESH
QT = 256
NEG = -1e30
NX = 4
PV = 768


def remote(src, dst, ss, rs, dev):
    return pltpu.make_async_remote_copy(
        src_ref=src, dst_ref=dst, send_sem=ss, recv_sem=rs, device_id=dev, device_id_type=MESH
    )


class ChipGather:
    def __init__(self, own, buf, core, right, left, partner, sems):
        ysend, yrecv, fsend, psend, precv = sems
        self.own, self.buf, self.core = own, buf, core
        self.out = {
            (s, p): remote(own[p], buf.at[s, core, p], ysend.at[s, p], yrecv.at[s, p], dev)
            for s, dev in ((1, right), (2, left))
            for p in (0, 1)
        }
        self.fwd = {
            (3, 0): remote(buf.at[1, core, 0], buf.at[3, core, 0], fsend.at[0], yrecv.at[3, 0], right),
            (3, 1): remote(buf.at[2, core, 1], buf.at[3, core, 1], fsend.at[1], yrecv.at[3, 1], left),
        }
        self.relay = {
            (s, p): remote(
                own[p] if s == 0 else buf.at[s, core, p], buf.at[s, core, p],
                psend.at[s, p], precv.at[s, p], partner,
            )
            for s in range(4)
            for p in (0, 1)
        }

    def start(self):
        for key in ((1, 0), (2, 1), (1, 1), (2, 0)):
            self.out[key].start()
        for p in (0, 1):
            self.relay[(0, p)].start()

    def arrive(self, slot, part, relay=True):
        (self.fwd if slot == 3 else self.out)[(slot, part)].wait_recv()
        if (slot, part) == (1, 0):
            self.fwd[(3, 0)].start()
        if (slot, part) == (2, 1):
            self.fwd[(3, 1)].start()
        if relay:
            self.relay[(slot, part)].start()

    def partner(self, slot, part):
        self.relay[(slot, part)].wait_recv()

    def drain(self):
        for c in list(self.out.values()) + list(self.fwd.values()) + list(self.relay.values()):
            c.wait_send()


def layer_kernel(
    rows, nz, nx, ny,
    tokens, norm_gain, query_gain, latent_gain, sinks, slopes,
    w_query, w_key, w_value, d_query, d_latent, w_rot, u_query, u_key, u_value, o_window, o_latent,
    tab_far, tab_near,
    result,
    tb, wb, wdq, wdl, wcat, wnarrow, uq, uk, uv, far, near, pacc, sq,
    kvm, qwt, kvw, osw, osl, orow,
    kvb, rotx, qb, kvp, mref, lref, acc,
    s00, s01, s10, s11, s20, s21, s30, s31, x00, x01, x10, x11, x20, x21, x30, x31, facc,
    osend, ssend, obuf, sbuf,
    l_sem, t_ysend, t_yrecv, t_fsend, t_psend, t_precv, w_ysend, w_yrecv, w_fsend, w_psend, w_precv,
    a_send, a_recv,
    h_send, h_recv, q_send, q_recv, qf_send, qf_recv, k_send, k_recv, kf_send, kf_recv,
    o_send, o_recv, s_send, s_recv,
):
    sp = lax.axis_index("sp")
    tp = lax.axis_index("tp")
    z, x = sp // nx, sp % nx
    y, core = tp // 2, tp % 2
    nsp, ntp = nz * nx, ny * 2
    tiles = rows // QT
    half_rows = rows // 2
    mine = rows // ntp

    loads = [
        pltpu.make_async_copy(s, d, l_sem.at[i])
        for i, (s, d) in enumerate((
            (d_query, wdq), (d_latent, wdl), (w_query, wcat.at[:, pl.ds(0, 128)]),
            (w_key, wnarrow.at[pl.ds(0, 64)]), (w_value, wnarrow.at[pl.ds(64, 64)]),
            (w_rot, wnarrow.at[pl.ds(128, 32)]), (u_query, uq), (u_key, uk), (u_value, uv),
            (tab_far.at[sp], far), (tab_near, near),
            (o_window, wb.at[0, core, 0]), (o_latent, wb.at[0, core, 1]),
        ))
    ]
    for c in loads:
        c.start()

    def at(zz, xx):
        return (zz * nx + xx, tp)

    def chip(step, cc):
        return (sp, ((y + step) % ny) * 2 + cc)

    xr, xl = at(z, (x + 1) % nx), at(z, (x + nx - 1) % nx)
    zr, zl, zo = at((z + 1) % nz, x), at((z + nz - 1) % nz, x), at((z + 2) % nz, x)
    nxt, prv = ((sp + 1) % nsp, tp), ((sp + nsp - 1) % nsp, tp)
    partner = chip(0, 1 - core)
    others = [chip(d, cc) for d in range(1, ny) for cc in (0, 1)] + [partner]

    barrier = pltpu.get_barrier_semaphore()
    peers = [xr, xl, zr, zl, zo, nxt, prv] + others
    for peer in peers:
        pl.semaphore_signal(barrier, inc=1, device_id=peer, device_id_type=MESH)
    pl.semaphore_wait(barrier, len(peers))

    tok = ChipGather(
        [tokens.at[pl.ds(p * half_rows, half_rows)] for p in (0, 1)], tb, core,
        chip(1, core), chip(ny - 1, core), partner, (t_ysend, t_yrecv, t_fsend, t_psend, t_precv),
    )
    wts = ChipGather(
        [o_window, o_latent], wb, core,
        chip(1, core), chip(ny - 1, core), partner, (w_ysend, w_yrecv, w_fsend, w_psend, w_precv),
    )
    tok.start()
    for p in (0, 1):
        tb[0, core, p] = tokens[p * half_rows : (p + 1) * half_rows]

    mref[...] = jnp.full(mref.shape, NEG, f32)
    lref[...] = jnp.zeros(lref.shape, f32)
    acc[...] = jnp.zeros(acc.shape, f32)
    ssend[...] = jnp.zeros(ssend.shape, f32)
    pacc[...] = jnp.zeros(pacc.shape, f32)
    sq[...] = jnp.zeros(sq.shape, f32)
    wnarrow[160:256] = jnp.zeros((96, D), bf16)
    for c in loads:
        c.wait()

    @pl.loop(0, D // 128)
    def _(b):
        at_b = pl.ds(pl.multiple_of(b * 128, 128), 128)
        wcat[at_b, 128:384] = wnarrow[:, at_b].astype(f32).T.astype(bf16)

    arrivals = {(1, 0): ((1, 0), (2, 1)), (1, 1): ((1, 1), (2, 0)), (3, 0): ((3, 0), (3, 1))}

    @pl.loop(0, 4)
    def _(slot):
        chip_at = (y + ny - (slot + slot // 2 - 2 * (slot // 3))) % ny
        w_rows = pl.ds(pl.multiple_of(chip_at * 512, 512), 512)

        @pl.loop(0, 2)
        def _(part):
            for s in range(4):
                for p in (0, 1):
                    @pl.when((slot == s) & (part == p))
                    def _():
                        for key in arrivals.get((s, p), ()):
                            tok.arrive(*key)
                        if (s, p) == (1, 1):
                            wts.start()
                        tok.partner(s, p)
            t32 = jnp.concatenate([tb[slot, 0, part], tb[slot, 1, part]], axis=1).astype(f32)
            out_rows = pl.ds(pl.multiple_of(part * half_rows, half_rows), half_rows)
            squares = t32 * t32
            sq[out_rows] += (
                squares[:, 0:128] + squares[:, 128:256] + squares[:, 256:384] + squares[:, 384:512]
            )
            scaled = (t32 * norm_gain[:, w_rows]).astype(bf16)
            for w, lo, hi in ((wdl, 768, 1280), (wcat, 1280, 1664), (wdq, 0, 768)):
                pacc[out_rows, lo:hi] += jnp.dot(scaled, w[w_rows, :], preferred_element_type=f32)

    cos_f, sin_f = far[0:16, 0:1], far[16:32, 0:1]
    cos_n, sin_n = near[0:16, :], near[16:32, :]
    cos = cos_f * cos_n - sin_f * sin_n
    sin = sin_f * cos_n + cos_f * sin_n
    near[0:16, :] = cos
    near[16:32, :] = sin
    row_scale = lax.rsqrt(jnp.sum(sq[...], axis=1, keepdims=True) * (1.0 / D) + EPS)

    def normed(lo, hi, gain):
        v = (pacc[:, lo:hi] * row_scale).astype(bf16).astype(f32)
        scale = lax.rsqrt(jnp.sum(v * v, axis=1, keepdims=True) * (1.0 / (hi - lo)) + EPS)
        return (v * scale * gain).astype(bf16)

    kvw[...] = (pacc[:, 1408:1536] * row_scale).astype(bf16)
    halo = [
        remote(kvw.at[pl.ds(rows - WINDOW, WINDOW)], kvp.at[pl.ds(0, WINDOW)], h_send.at[0], h_recv.at[0], nxt),
        remote(kvw.at[pl.ds(0, WINDOW)], kvp.at[pl.ds(rows + WINDOW, WINDOW)], h_send.at[1], h_recv.at[1], prv),
    ]
    for c in halo:
        c.start()
    quarter = rows // 4
    up_kv = jnp.concatenate([uk[...], uv[...]], axis=1)
    kv = jnp.dot(normed(768, 1280, latent_gain[...]), up_kv, preferred_element_type=f32)
    kvm[0:rows] = kv[:, 0:128].astype(bf16)
    for b in range(rows // 128):
        block = kv[128 * b : 128 * b + 128, 128:256].T
        kvm[rows + quarter + 128 * b : rows + quarter + 128 * b + 128] = block.astype(bf16)
    rr = (pacc[:, 1536:1664] * row_scale).astype(bf16).astype(f32).T
    ra, rb = rr[0:16], rr[16:32]
    cos, sin = near[0:16, :], near[16:32, :]
    turned = jnp.concatenate([ra * cos - rb * sin, rb * cos + ra * sin, jnp.zeros((96, rows), f32)], axis=0).T
    packed = turned[0:quarter]
    for g in range(1, 4):
        packed = packed + pltpu.roll(turned[g * quarter : (g + 1) * quarter], 32 * g, 1)
    kvm[rows : rows + quarter] = packed.astype(bf16)
    half = kvm.shape[0] // 2
    k_out = {}
    for order in ((0, 1), (1, 0)):
        for which, h in ((0, order[0]), (1, order[1])):
            slot, dev = ((1, xr), (2, xl))[which]
            k_out[(which, h)] = remote(
                kvm.at[pl.ds(h * half, half)], kvb.at[slot, pl.ds(h * half, half)],
                k_send.at[which, h], k_recv.at[which, h], dev,
            )
    for key in ((0, 0), (1, 1), (0, 1), (1, 0)):
        k_out[key].start()
    kvb[0] = kvm[...]

    qf = lax.dot_general(
        uq[...], normed(0, 768, jnp.concatenate([query_gain[i : i + 1] for i in range(6)], axis=1)), (((1,), (1,)), ((), ())), preferred_element_type=f32
    ) * (LOG2E * 96 ** (-0.5))
    for h in range(2):
        a, b = qf[96 * h + 64 : 96 * h + 80], qf[96 * h + 80 : 96 * h + 96]
        whole = jnp.concatenate(
            [qf[96 * h : 96 * h + 64], a * cos - b * sin, b * cos + a * sin], axis=0
        ).astype(bf16)
        for t in range(tiles):
            qb[0, t, h] = whole[:, QT * t : QT * t + QT]
    q_out = {
        (slot, t): remote(qb.at[0, t], qb.at[slot, t], q_send.at[slot, t], q_recv.at[slot, t], dev)
        for t in range(tiles)
        for slot, dev in ((1, zr), (2, zl))
    }
    for c in q_out.values():
        c.start()
    q_fwd = {}
    for n in range(2 * tiles):
        t, h = n // 2, n % 2
        slot, dev = (1, zr) if n < tiles else (2, zl)
        q_fwd[(t, h)] = remote(qb.at[slot, t, h], qb.at[3, t, h], qf_send.at[t, h], qf_recv.at[t, h], dev)

    kvp[WINDOW : WINDOW + rows] = kvw[...]
    wq = pacc[:, 1280:1408] * row_scale
    for t in range(tiles):
        qwt[t] = wq[QT * t : QT * t + QT].T.astype(bf16).reshape(2, 64, QT)
    k_fwd = [
        remote(kvb.at[1, pl.ds(0, half)], kvb.at[3, pl.ds(0, half)], kf_send.at[0], kf_recv.at[0], xr),
        remote(kvb.at[2, pl.ds(half, half)], kvb.at[3, pl.ds(half, half)], kf_send.at[1], kf_recv.at[1], xl),
    ]

    def unpack(i):
        packed = kvb[i, rows : rows + quarter].astype(f32)
        for g in range(4):
            moved = packed if g == 0 else pltpu.roll(packed, 128 - 32 * g, 1)
            rotx[i, g * quarter : (g + 1) * quarter] = moved.astype(bf16)

    def piece(part, src, d, cc):
        dev = chip(d, cc) if d else partner
        slot = (0, 1, 3, 2)[d]
        row_at = pl.ds(pl.multiple_of(dev[1] * mine, mine), mine)
        i = 2 * d + (cc if d else 0)
        return remote(
            src.at[row_at], orow.at[slot, core, part], a_send.at[part, i], a_recv.at[part, slot, core], dev
        )

    def pieces(part, src):
        keys = [(2, 0), (2, 1), (1, 0), (3, 0), (1, 1), (3, 1), (0, 0)]
        return [piece(part, src, d, cc) for d, cc in keys]

    S = ((s00, s01), (s10, s11), (s20, s21), (s30, s31))
    X = ((x00, x01), (x10, x11), (x20, x21), (x30, x31))

    def stage_a(k, q, t, slot, h):
        z64, z96 = jnp.zeros((64, QT), bf16), jnp.zeros((96, QT), bf16)
        keys = jnp.concatenate([kvb[k, 0:rows], rotx[k]], axis=1)
        qq = qb[q, t, h]
        parts = [z64, z64, qq[64:96], z96]
        parts[h] = qq[0:64]
        s = jnp.dot(keys, jnp.concatenate(parts, axis=0), preferred_element_type=f32)
        S[slot][h][...] = s
        X[slot][h][...] = jnp.max(s.reshape(rows // 8, 8, QT), axis=0)

    def stage_b(k, q, t, slot, h):
        old = mref[q, t, h : h + 1]
        new = jnp.maximum(old, jnp.max(X[slot][h][...], axis=0, keepdims=True))
        alpha = jnp.exp2(old - new)
        mref[q, t, h : h + 1] = new
        total = None
        for lo in range(0, rows, PV):
            hi = min(rows, lo + PV)
            p = jnp.exp2(S[slot][h][lo:hi] - new).astype(bf16)
            base = rows + quarter + 64 * h
            v = jnp.concatenate([kvb[k, base + c : base + c + 64] for c in range(lo, hi, 128)], axis=1)
            v = jnp.concatenate([v, jnp.ones((16, hi - lo), bf16)], axis=0)
            o = jnp.dot(v, p, preferred_element_type=f32)
            total = o if total is None else total + o
        lref[q, t, h : h + 1] = lref[q, t, h : h + 1] * alpha + total[64:65]
        acc[q, t, 64 * h : 64 * h + 64] = acc[q, t, 64 * h : 64 * h + 64] * alpha + total[0:64]

    def pipeline(n, where, before=None, after=None):
        def step(first, second):
            for i, _ in first:
                if before is not None:
                    before(i)
            for d in range(2):
                for h in range(2):
                    if d < len(first):
                        i, slot = first[d]
                        stage_a(*where(i), slot, h)
                    if d < len(second):
                        i, slot = second[d]
                        stage_b(*where(i), slot, h)
            for i, _ in second:
                if after is not None:
                    after(i)

        def body(i, at):
            step(
                [(i + 2, (at + 2) % 4), (i + 3, (at + 3) % 4)], [(i, at), (i + 1, at + 1)]
            )

        step([(0, 0), (1, 1)], [])
        bodies = n // 2 - 1
        loops = bodies // 2
        if loops == 1:
            body(0, 0)
            body(2, 2)
        elif loops:
            @pl.loop(0, loops)
            def _(j):
                body(4 * j, 0)
                body(4 * j + 2, 2)
        if bodies % 2:
            body(4 * loops, 0)
        i = 2 * bodies
        last = [(i, i % 4), (i + 1, (i + 1) % 4)]
        if n % 2:
            step([(i + 2, (i + 2) % 4)], last)
            last = [(i + 2, (i + 2) % 4)]
        step([], last)

    def window():
        for c in halo:
            c.wait_recv()
        span = QT + 2 * WINDOW
        key_i = lax.broadcasted_iota(jnp.int32, (span, QT), 0)
        dist = key_i - WINDOW - lax.broadcasted_iota(jnp.int32, (span, QT), 1)
        dist = jnp.abs(dist)
        distf = dist.astype(f32)

        @pl.loop(0, tiles)
        def _(t):
            rows_at = pl.ds(pl.multiple_of(t * QT, QT), span)
            kv = kvp[rows_at]
            pos = sp * rows + t * QT + key_i - WINDOW
            valid = (dist <= WINDOW) & (pos >= 0) & (pos < nsp * rows)
            for h in range(2):
                slope, sink = slopes[tp * 2 + h], sinks[h]
                rhs = jnp.concatenate([qwt[t, h], jnp.zeros((64, QT), bf16)], axis=0)
                s = jnp.dot(kv, rhs, preferred_element_type=f32) * 0.125
                s = jnp.where(valid, s - slope * distf, NEG)
                m = jnp.maximum(jnp.max(s, axis=0, keepdims=True), sink)
                w = jnp.exp2((s - m) * LOG2E)
                denom = jnp.sum(w, axis=0, keepdims=True) + jnp.exp2((sink - m) * LOG2E)
                w = (w * (1.0 / denom)).astype(bf16)
                o = lax.dot_general(kv, w, (((0,), (0,)), ((), ())), preferred_element_type=f32)
                S[0][0][h * 64 : h * 64 + 64] = o[64:128]
            osw[pl.ds(pl.multiple_of(t * QT, QT), QT), :] = S[0][0][0:128].T.astype(bf16)

    unpack(0)
    pipeline(tiles, lambda i: (0, 0, i))
    window()
    for c in pieces(0, osw):
        c.start()
    orow[0, core, 0] = osw[pl.ds(pl.multiple_of(tp * mine, mine), mine), :]

    def queries_arrive(i):
        if i % 2 == 0:
            t = i // 2
            q_out[(1, t)].wait_recv()
            q_out[(2, t)].wait_recv()
            for h in range(2):
                q_fwd[(t, h)].start()
            if t == tiles - 1:
                for c, f in ((k_out[(0, 0)], k_fwd[0]), (k_out[(1, 1)], k_fwd[1])):
                    c.wait_recv()
                    f.start()

    pipeline(2 * tiles, lambda i: (0, 1 + i % 2, i // 2), queries_arrive)

    k_out[(0, 1)].wait_recv()
    k_out[(1, 0)].wait_recv()
    unpack(1)
    unpack(2)
    for c in q_fwd.values():
        c.wait_recv()
    wts.arrive(1, 0)
    wts.arrive(2, 1)

    def arrive(i):
        @pl.when(i == 5 * tiles)
        def _():
            for c in k_fwd:
                c.wait_recv()
            unpack(3)

        @pl.when(i == 6 * tiles)
        def _():
            wts.arrive(1, 1)
            wts.arrive(2, 0)

    def finish(q, t):
        for h in range(2):
            inv = 1.0 / lref[q, t, h : h + 1]
            osend[q, t, 64 * h : 64 * h + 64] = (acc[q, t, 64 * h : 64 * h + 64] * inv).astype(bf16)
        ssend[q, t, 0:2] = mref[q, t, 0:2]
        ssend[q, t, 2:4] = lref[q, t, 0:2]

    def back(q, t):
        slot, dev = {3: (3, zo), 2: (1, zr), 1: (2, zl)}[q]
        return (
            remote(osend.at[q, t], obuf.at[slot, t], o_send.at[q, t], o_recv.at[slot, t], dev),
            remote(ssend.at[q, t], sbuf.at[slot, t], s_send.at[q, t], s_recv.at[slot, t], dev),
        )

    def mixed_order(i):
        p = i // tiles
        return p - 2 * (p // 3) + p // 6, 3 - p // 3 + p // 5, i % tiles

    def give_back(i):
        for q in (3, 2):
            @pl.when(i // tiles == 8 - q)
            def _():
                finish(q, i % tiles)
                for c in back(q, i % tiles):
                    c.start()

    pipeline(7 * tiles, mixed_order, arrive, give_back)

    def by_tile(i):
        return 1 + i % 3, 1 - i // (3 * tiles), (i % (3 * tiles)) // 3

    def give_back_last(i):
        @pl.when(i % 3 == 2)
        def _():
            _, q, t = by_tile(i)
            finish(q, t)

            @pl.when(i < 3 * tiles)
            def _():
                for c in back(1, t):
                    c.start()

    pipeline(6 * tiles, by_tile, None, give_back_last)

    for q in (3, 2, 1):
        for t in range(tiles):
            for c in back(q, t):
                c.wait_recv()

    @pl.loop(0, tiles)
    def _(t):
        ms = [ssend[0, t, 0:2]] + [sbuf[j, t, 0:2] for j in (1, 2, 3)]
        ls = [ssend[0, t, 2:4]] + [sbuf[j, t, 2:4] for j in (1, 2, 3)]
        top = jnp.maximum(jnp.maximum(ms[0], ms[1]), jnp.maximum(ms[2], ms[3]))
        ws = [l * jnp.exp2(m - top) for m, l in zip(ms, ls)]
        inv = 1.0 / (ws[0] + ws[1] + ws[2] + ws[3])
        for h in range(2):
            rows_h = slice(64 * h, 64 * h + 64)
            total = osend[0, t, rows_h].astype(f32) * (ws[0] * inv)[h : h + 1]
            for j in (1, 2, 3):
                total = total + obuf[j, t, rows_h].astype(f32) * (ws[j] * inv)[h : h + 1]
            S[0][0][rows_h] = total
        osl[pl.ds(pl.multiple_of(t * QT, QT), QT), :] = S[0][0][0:128].T.astype(bf16)

    for c in pieces(1, osl):
        c.start()
    orow[0, core, 1] = osl[pl.ds(pl.multiple_of(tp * mine, mine), mine), :]
    wts.arrive(3, 0)
    wts.arrive(3, 1)

    def output(slots, last):
        for s in slots:
            for p in (0, 1):
                wts.partner(s, p)
                for cc in (0, 1) if s else (1 - core,):
                    there = orow.at[s, cc, p]
                    remote(there, there, a_send.at[p, 0], a_recv.at[p, s, cc], partner).wait_recv()

        @pl.loop(0, D // 512)
        def _(b):
            cols = pl.ds(pl.multiple_of(b * 512, 512), 512)
            total = facc[:, cols] if last else None
            for s in slots:
                for cc in (0, 1):
                    o = jnp.concatenate([orow[s, cc, 0], orow[s, cc, 1]], axis=1)
                    w = jnp.concatenate([wb[s, cc, 0, :, cols], wb[s, cc, 1, :, cols]], axis=0)
                    g = jnp.dot(o, w, preferred_element_type=f32).astype(bf16).astype(f32)
                    total = g if total is None else total + g
            if last:
                result[:, cols] = total.astype(bf16)
            else:
                facc[:, cols] = total

    output((0, 1, 2), False)
    output((3,), True)

    for c in halo + list(q_out.values()) + list(k_out.values()) + list(q_fwd.values()) + k_fwd:
        c.wait_send()
    for q in (3, 2, 1):
        for t in range(tiles):
            for c in back(q, t):
                c.wait_send()
    for part, src in ((0, osw), (1, osl)):
        for c in pieces(part, src):
            c.wait_send()
    tok.drain()
    wts.drain()


def angle_tables(rows, nsp):
    inverse = THETA ** (-np.arange(16, dtype=np.float64) / 16)
    far = np.arange(nsp)[:, None] * rows * inverse[None, :]
    far = np.concatenate([np.cos(far), np.sin(far)], axis=1)[:, :, None]
    near = inverse[:, None] * np.arange(rows)[None, :]
    near = np.concatenate([np.cos(near), np.sin(near)], axis=0)
    return np.broadcast_to(far, (nsp, 32, 128)).astype(np.float32), near.astype(np.float32)


def per_device(
    nsp, ntp, tokens, norm_gain, window_query, window_key, window_value, sink_logit, down_query,
    down_latent, rotary_proj, query_gain, latent_gain, up_query, up_key, up_value, window_out, latent_out,
):
    rows = tokens.shape[0]
    tiles, mine, half_rows = rows // QT, rows // ntp, rows // 2
    far, near = angle_tables(rows, nsp)
    slopes = np.exp2(-8.0 * (np.arange(A_HEADS) + 1.0) / A_HEADS).astype(np.float32)
    dma, V = pltpu.SemaphoreType.DMA, pltpu.VMEM
    vm, smem = pl.BlockSpec(memory_space=pltpu.VMEM), pl.BlockSpec(memory_space=pltpu.SMEM)
    hbm = pl.BlockSpec(memory_space=pl.ANY)
    gather_sems = [dma((3, 2)), dma((4, 2)), dma((2,)), dma((4, 2)), dma((4, 2))]
    message = rows + rows // 4 + rows
    return pl.pallas_call(
        functools.partial(layer_kernel, rows, nsp // NX, NX, ntp // 2),
        out_shape=jax.ShapeDtypeStruct((mine, D), bf16),
        in_specs=[vm, vm, vm, vm, smem, smem] + [hbm] * 13,
        out_specs=vm,
        scratch_shapes=[
            V((4, 2, 2, half_rows, 256), bf16), V((4, 2, 2, 128, D), bf16),
            V((D, 768), bf16), V((D, 512), bf16), V((D, 384), bf16),
            V((256, D), bf16),
            V((192, 768), bf16), V((512, 128), bf16), V((512, 128), bf16),
            V((32, 128), f32), V((32, rows), f32), V((rows, 1664), f32), V((rows, 128), f32),
            V((message, 128), bf16), V((tiles, 2, 64, QT), bf16), V((rows, 128), bf16),
            V((rows, 128), bf16), V((rows, 128), bf16), V((4, 2, 2, mine, 128), bf16),
            V((4, message, 128), bf16), V((4, rows, 128), bf16), V((4, tiles, 2, 96, QT), bf16),
            V((rows + 2 * WINDOW, 128), bf16),
            V((4, tiles, 8, QT), f32), V((4, tiles, 8, QT), f32), V((4, tiles, 128, QT), f32),
        ]
        + [V((rows, QT), f32)] * 8 + [V((8, QT), f32)] * 8 + [V((mine, D), f32)]
        + [
            V((4, tiles, 128, QT), bf16), V((4, tiles, 8, QT), f32),
            V((4, tiles, 128, QT), bf16), V((4, tiles, 8, QT), f32),
            dma((13,)),
        ]
        + gather_sems + gather_sems
        + [
            dma((2, 8)), dma((2, 4, 2)),
            dma((2,)), dma((2,)), dma((3, tiles)), dma((3, tiles)), dma((tiles, 2)), dma((tiles, 2)),
            dma((2, 2)), dma((2, 2)), dma((2,)), dma((2,)),
            dma((4, tiles)), dma((4, tiles)), dma((4, tiles)), dma((4, tiles)),
        ],
        compiler_params=pltpu.CompilerParams(
            collective_id=1, has_side_effects=True, vmem_limit_bytes=60 * 2**20
        ),
        name="layer",
    )(
        tokens, norm_gain.reshape(1, D), query_gain.reshape(6, 128), latent_gain.reshape(1, -1),
        sink_logit, jnp.asarray(slopes), window_query, window_key.T, window_value.T, down_query, down_latent,
        rotary_proj.T, up_query.T, up_key, up_value, window_out, latent_out, jnp.asarray(far), jnp.asarray(near),
    )


def solution(mesh):
    col, row, rep = P(None, "tp"), P("tp", None), P()
    placed = (
        P("sp", "tp"), rep, col, col, col, P("tp"), rep, rep, rep, rep, rep, col, col, col, row, row,
    )
    body = functools.partial(per_device, mesh.shape["sp"], mesh.shape["tp"])
    return jax.shard_map(
        body, mesh=mesh, in_specs=placed, out_specs=P(("sp", "tp"), None), check_vma=False
    )
```

```python
import functools
import jax
import jax.numpy as jnp
import numpy as np
from jax import lax
from jax.experimental import pallas as pl
from jax.experimental.pallas import tpu as pltpu
from jax.sharding import PartitionSpec as P

D = 2048
A_HEADS = 16
WINDOW = 128
EPS = 1e-06
THETA = 10000.0
LOG2E = 1.4426950408889634
f32, bf16 = jnp.float32, jnp.bfloat16
MESH = pl.DeviceIdType.MESH
QT = 256
NEG = -1e30
NX = 4
PV = 768
CB = 512


def remote(src, dst, ss, rs, dev):
    return pltpu.make_async_remote_copy(
        src_ref=src, dst_ref=dst, send_sem=ss, recv_sem=rs, device_id=dev, device_id_type=MESH
    )


class ChipGather:
    def __init__(self, own, buf, core, right, left, partner, sems, keep):
        ysend, yrecv, fsend, psend, precv = sems
        self.own, self.buf, self.core = own, buf, core
        size = buf.shape[3]
        head, rest = pl.ds(0, keep), pl.ds(keep, size - keep)
        self.out = {
            (s, p): remote(own[p], buf.at[s, core, p], ysend.at[s, p], yrecv.at[s, p], dev)
            for s, dev in ((1, right), (2, left))
            for p in (0, 1)
        }
        self.fwd = {
            (3, 0): remote(
                buf.at[1, core, 0, head], buf.at[3, core, 0, head], fsend.at[0], yrecv.at[3, 0], right
            ),
            (3, 1): remote(buf.at[2, core, 1], buf.at[3, core, 1], fsend.at[1], yrecv.at[3, 1], left),
        }
        self.more = []
        if keep < size:
            self.more = [
                remote(buf.at[2, core, 0, rest], buf.at[3, core, 0, rest], fsend.at[2], yrecv.at[0, 0], left)
            ]
        self.relay = {
            (s, p): remote(
                own[p] if s == 0 else buf.at[s, core, p], buf.at[s, core, p],
                psend.at[s, p], precv.at[s, p], partner,
            )
            for s in range(4)
            for p in (0, 1)
        }

    def start(self):
        for key in ((1, 0), (2, 1), (1, 1), (2, 0)):
            self.out[key].start()
        for p in (0, 1):
            self.relay[(0, p)].start()

    def arrive(self, slot, part, relay=True):
        (self.fwd if slot == 3 else self.out)[(slot, part)].wait_recv()
        if (slot, part) == (1, 0):
            self.fwd[(3, 0)].start()
        if (slot, part) == (2, 1):
            self.fwd[(3, 1)].start()
        if (slot, part) == (2, 0):
            for c in self.more:
                c.start()
        if (slot, part) == (3, 0):
            for c in self.more:
                c.wait_recv()
        if relay:
            self.relay[(slot, part)].start()

    def partner(self, slot, part):
        self.relay[(slot, part)].wait_recv()

    def drain(self):
        for c in list(self.out.values()) + list(self.fwd.values()) + self.more + list(self.relay.values()):
            c.wait_send()


class WeightGather:
    def __init__(self, buf, core, a, right, left, partner, across, sems):
        osend, orecv, fsend, frecv, xsend, xrecv, psend, precv = sems
        rows = buf.shape[3]
        b, cut, mid = 1 - a, rows // 4, rows // 2
        chunks = ((a, pl.ds(0, rows)), (b, pl.ds(0, cut)), (b, pl.ds(cut, rows - cut)))
        self.out = {
            (s, i): remote(
                buf.at[0, core, p, r], buf.at[s, core, p, r], osend.at[s, i], orecv.at[s, i], dev
            )
            for s, dev in ((1, right), (2, left))
            for i, (p, r) in enumerate(chunks)
        }
        self.fwd = [
            remote(buf.at[s, core, a, r], buf.at[3, core, a, r], fsend.at[i], frecv.at[i], dev)
            for i, (s, dev, r) in enumerate(((1, right, pl.ds(0, mid)), (2, left, pl.ds(mid, rows - mid))))
        ]
        self.swap = remote(buf.at[3, core, a], buf.at[3, core, a], xsend.at[0], xrecv.at[0], across)
        self.relay = {
            (s, i): remote(
                buf.at[s, core, p], buf.at[s, core, p], psend.at[s, i], precv.at[s, i], partner
            )
            for s in range(4)
            for i, p in enumerate((a, b))
        }

    def start(self):
        for key in ((1, 0), (2, 0), (1, 1), (2, 1)):
            self.out[key].start()
        for i in (0, 1):
            self.relay[(0, i)].start()

    def first(self):
        for s in (1, 2):
            self.out[(s, 0)].wait_recv()
            self.fwd[s - 1].start()
        for s in (1, 2):
            self.out[(s, 2)].start()
            self.relay[(s, 0)].start()

    def second(self):
        for c in self.fwd:
            c.wait_recv()
        self.swap.start()
        self.relay[(3, 0)].start()

    def third(self):
        for s in (1, 2):
            self.out[(s, 1)].wait_recv()
            self.out[(s, 2)].wait_recv()
            self.relay[(s, 1)].start()

    def fourth(self):
        self.swap.wait_recv()
        self.relay[(3, 1)].start()

    def partner(self, slot, part):
        self.relay[(slot, part)].wait_recv()

    def drain(self):
        for c in list(self.out.values()) + self.fwd + [self.swap] + list(self.relay.values()):
            c.wait_send()


def layer_kernel(
    rows, nz, nx, ny,
    tokens, norm_gain, query_gain, latent_gain, sinks, slopes,
    w_query, w_key, w_value, d_query, d_latent, w_rot, u_query, u_key, u_value, o_window, o_latent,
    tab_far, tab_near, tab_near_q,
    result,
    tb, wb, wdq, wdl, wcat, wnarrow, uq, uk, uv, far, near, near_q, pacc, sq,
    kvm, qwt, kvw, osw, osl, orow,
    kvb, rotx, qb, kvp, mref, lref, acc,
    s00, s01, s10, s11, s20, s21, s30, s31, x00, x01, x10, x11, x20, x21, x30, x31, facc, total_out,
    osend, ssend, obuf, sbuf,
    l_sem, t_ysend, t_yrecv, t_fsend, t_psend, t_precv, w_osend, w_orecv, w_fsend, w_frecv, w_xsend, w_xrecv, w_psend, w_precv,
    a_send, a_recv, r_sem,
    h_send, h_recv, q_send, q_recv, qf_send, qf_recv, k_send, k_recv, kf_send, kf_recv,
    o_send, o_recv, s_send, s_recv,
):
    sp = lax.axis_index("sp")
    tp = lax.axis_index("tp")
    z, x = sp // nx, sp % nx
    y, core = tp // 2, tp % 2
    nsp, ntp = nz * nx, ny * 2
    tiles = rows // QT
    half_rows = rows // 2
    mine = rows // ntp

    loads = [
        pltpu.make_async_copy(s, d, l_sem.at[i])
        for i, (s, d) in enumerate((
            (d_query, wdq), (d_latent, wdl), (w_query, wcat.at[:, pl.ds(0, 128)]),
            (w_key, wnarrow.at[pl.ds(0, 64)]), (w_value, wnarrow.at[pl.ds(64, 64)]),
            (w_rot, wnarrow.at[pl.ds(128, 32)]), (u_query, uq), (u_key, uk), (u_value, uv),
            (tab_far.at[sp], far), (tab_near, near), (tab_near_q, near_q),
            (o_window, wb.at[0, core, 0]), (o_latent, wb.at[0, core, 1]),
        ))
    ]
    for c in loads:
        c.start()

    def at(zz, xx):
        return (zz * nx + xx, tp)

    def chip(step, cc):
        return (sp, ((y + step) % ny) * 2 + cc)

    xr, xl = at(z, (x + 1) % nx), at(z, (x + nx - 1) % nx)
    zr, zl, zo = at((z + 1) % nz, x), at((z + nz - 1) % nz, x), at((z + 2) % nz, x)
    nxt, prv = ((sp + 1) % nsp, tp), ((sp + nsp - 1) % nsp, tp)
    partner = chip(0, 1 - core)
    others = [chip(d, cc) for d in range(1, ny) for cc in (0, 1)] + [partner]

    barrier = pltpu.get_barrier_semaphore()
    peers = [xr, xl, zr, zl, zo, nxt, prv] + others
    for peer in peers:
        pl.semaphore_signal(barrier, inc=1, device_id=peer, device_id_type=MESH)
    pl.semaphore_wait(barrier, len(peers))

    tok = ChipGather(
        [tokens.at[pl.ds(p * half_rows, half_rows)] for p in (0, 1)], tb, core,
        chip(1, core), chip(ny - 1, core), partner, (t_ysend, t_yrecv, t_fsend, t_psend, t_precv), half_rows,
    )
    wts = WeightGather(
        wb, core, x % 2, chip(1, core), chip(ny - 1, core), partner, at(z, x + 1 - 2 * (x % 2)),
        (w_osend, w_orecv, w_fsend, w_frecv, w_xsend, w_xrecv, w_psend, w_precv),
    )
    tok.start()
    for p in (0, 1):
        tb[0, core, p] = tokens[p * half_rows : (p + 1) * half_rows]

    mref[...] = jnp.full(mref.shape, NEG, f32)
    lref[...] = jnp.zeros(lref.shape, f32)
    acc[...] = jnp.zeros(acc.shape, f32)
    ssend[...] = jnp.zeros(ssend.shape, f32)
    pacc[...] = jnp.zeros(pacc.shape, f32)
    sq[...] = jnp.zeros(sq.shape, f32)
    wnarrow[160:256] = jnp.zeros((96, D), bf16)
    for c in loads:
        c.wait()

    @pl.loop(0, D // 128)
    def _(b):
        at_b = pl.ds(pl.multiple_of(b * 128, 128), 128)
        wcat[at_b, 128:384] = wnarrow[:, at_b].astype(f32).T.astype(bf16)

    arrivals = {(1, 0): ((1, 0), (2, 1)), (1, 1): ((1, 1), (2, 0))}

    all_parts = ((wdl, 768, 1280), (wcat, 1280, 1664), (wdq, 0, 768))

    def unit(t32, w_rows, out_rows, parts=all_parts, count=True):
        if count:
            squares = t32 * t32
            part_sq = squares[:, 0:128]
            for lo in range(128, t32.shape[1], 128):
                part_sq = part_sq + squares[:, lo : lo + 128]
            sq[out_rows] += part_sq
        scaled = (t32 * norm_gain[:, w_rows]).astype(bf16)
        for w, lo, hi in parts:
            pacc[out_rows, lo:hi] += jnp.dot(scaled, w[w_rows, :], preferred_element_type=f32)

    @pl.loop(0, 3)
    def _(slot):
        chip_at = (y + ny - (slot + slot // 2)) % ny
        w_rows = pl.ds(pl.multiple_of(chip_at * 512, 512), 512)

        @pl.loop(0, 2)
        def _(part):
            for s in range(3):
                for p in (0, 1):
                    @pl.when((slot == s) & (part == p))
                    def _():
                        for key in arrivals.get((s, p), ()):
                            tok.arrive(*key)
                        if (s, p) == (1, 1):
                            wts.start()
                        tok.partner(s, p)
            out_rows = pl.ds(pl.multiple_of(part * half_rows, half_rows), half_rows)
            t32 = jnp.concatenate([tb[slot, 0, part], tb[slot, 1, part]], axis=1).astype(f32)
            unit(t32, w_rows, out_rows)

    tok.arrive(3, 0)
    tok.arrive(3, 1)

    @pl.loop(0, 2)
    def _(turn):
        from_core = core + turn - 2 * core * turn

        @pl.when(turn == 1)
        def _():
            tok.partner(3, 0)
            tok.partner(3, 1)

        @pl.loop(0, 2)
        def _(part):
            w_rows = pl.ds(pl.multiple_of(((y + 2) % ny) * 512 + from_core * 256, 256), 256)
            out_rows = pl.ds(pl.multiple_of(part * half_rows, half_rows), half_rows)
            unit(tb[3, from_core, part].astype(f32), w_rows, out_rows, all_parts[:2])

    cos_f, sin_f = far[0:16, 0:1], far[16:32, 0:1]
    for table in (near, near_q):
        cos_n, sin_n = table[0:16, :], table[16:32, :]
        cos, sin = cos_f * cos_n - sin_f * sin_n, sin_f * cos_n + cos_f * sin_n
        table[0:16, :] = cos
        table[16:32, :] = sin
    row_scale = lax.rsqrt(jnp.sum(sq[...], axis=1, keepdims=True) * (1.0 / D) + EPS)

    def normed(lo, hi, gain):
        v = (pacc[:, lo:hi] * row_scale).astype(bf16).astype(f32)
        scale = lax.rsqrt(jnp.sum(v * v, axis=1, keepdims=True) * (1.0 / (hi - lo)) + EPS)
        return (v * scale * gain).astype(bf16)

    kvw[...] = (pacc[:, 1408:1536] * row_scale).astype(bf16)
    halo = [
        remote(kvw.at[pl.ds(rows - WINDOW, WINDOW)], kvp.at[pl.ds(0, WINDOW)], h_send.at[0], h_recv.at[0], nxt),
        remote(kvw.at[pl.ds(0, WINDOW)], kvp.at[pl.ds(rows + WINDOW, WINDOW)], h_send.at[1], h_recv.at[1], prv),
    ]
    for c in halo:
        c.start()
    quarter, eighth = rows // 4, rows // 8
    half = kvm.shape[0] // 2
    v_at = half_rows + eighth

    def value_row(c):
        return (c // half_rows) * half + v_at + c % half_rows

    up_kv = jnp.concatenate([uk[...], uv[...]], axis=1)
    kv = jnp.dot(normed(768, 1280, latent_gain[...]), up_kv, preferred_element_type=f32)
    for e in (0, 1):
        kvm[e * half : e * half + half_rows] = kv[e * half_rows : (e + 1) * half_rows, 0:128].astype(bf16)
    for b in range(rows // 128):
        block = kv[128 * b : 128 * b + 128, 128:256].T
        kvm[value_row(128 * b) : value_row(128 * b) + 128] = block.astype(bf16)
    rr = (pacc[:, 1536:1664] * row_scale).astype(bf16).astype(f32).T
    ra, rb = rr[0:16], rr[16:32]
    cos, sin = near[0:16, :], near[16:32, :]
    turned = jnp.concatenate([ra * cos - rb * sin, rb * cos + ra * sin, jnp.zeros((96, rows), f32)], axis=0).T
    for e in (0, 1):
        packed = turned[e * half_rows : e * half_rows + eighth]
        for g in range(1, 4):
            lo = e * half_rows + g * eighth
            packed = packed + pltpu.roll(turned[lo : lo + eighth], 32 * g, 1)
        kvm[e * half + half_rows : e * half + v_at] = packed.astype(bf16)
    k_out = {}
    for order in ((0, 1), (1, 0)):
        for which, h in ((0, order[0]), (1, order[1])):
            slot, dev = 1 if which == h else 2, (xr, xl)[which]
            k_out[(which, h)] = remote(
                kvm.at[pl.ds(h * half, half)], kvb.at[slot, pl.ds(h * half, half)],
                k_send.at[which, h], k_recv.at[which, h], dev,
            )
    for key in ((0, 0), (1, 1), (0, 1), (1, 0)):
        k_out[key].start()
    kvb[0] = kvm[...]

    @pl.loop(0, 2)
    def _(part):
        w_rows = pl.ds(pl.multiple_of(((y + 2) % ny) * 512, 512), 512)
        out_rows = pl.ds(pl.multiple_of(part * half_rows, half_rows), half_rows)
        t32 = jnp.concatenate([tb[3, 0, part], tb[3, 1, part]], axis=1).astype(f32)
        unit(t32, w_rows, out_rows, all_parts[2:], False)

    sub = mine // tiles
    nq = normed(0, 768, jnp.concatenate([query_gain[i : i + 1] for i in range(6)], axis=1))
    nq = jnp.concatenate(
        [nq[mine * j + sub * t : mine * j + sub * t + sub] for t in range(tiles) for j in range(ntp)], axis=0
    )
    qf = lax.dot_general(uq[...], nq, (((1,), (1,)), ((), ())), preferred_element_type=f32) * (LOG2E * 96 ** (-0.5))
    cos, sin = near_q[0:16, :], near_q[16:32, :]
    for h in range(2):
        a, b = qf[96 * h + 64 : 96 * h + 80], qf[96 * h + 80 : 96 * h + 96]
        whole = jnp.concatenate(
            [qf[96 * h : 96 * h + 64], a * cos - b * sin, b * cos + a * sin], axis=0
        ).astype(bf16)
        for t in range(tiles):
            qb[0, t, h] = whole[:, QT * t : QT * t + QT]
    q_out = {
        (slot, t): remote(qb.at[0, t], qb.at[slot, t], q_send.at[slot, t], q_recv.at[slot, t], dev)
        for t in range(tiles)
        for slot, dev in ((1, zr), (2, zl))
    }
    for c in q_out.values():
        c.start()
    q_fwd = {}
    for n in range(2 * tiles):
        t, h = n // 2, n % 2
        slot, dev = (1, zr) if n < tiles else (2, zl)
        q_fwd[(t, h)] = remote(qb.at[slot, t, h], qb.at[3, t, h], qf_send.at[t, h], qf_recv.at[t, h], dev)

    kvp[WINDOW : WINDOW + rows] = kvw[...]
    wq = pacc[:, 1280:1408] * row_scale
    for t in range(tiles):
        qwt[t] = wq[QT * t : QT * t + QT].T.astype(bf16).reshape(2, 64, QT)
    k_fwd = [
        remote(kvb.at[1, pl.ds(0, half)], kvb.at[3, pl.ds(0, half)], kf_send.at[0], kf_recv.at[0], xr),
        remote(kvb.at[1, pl.ds(half, half)], kvb.at[3, pl.ds(half, half)], kf_send.at[1], kf_recv.at[1], xl),
    ]

    def unpack(i):
        for e in (0, 1):
            packed = kvb[i, e * half + half_rows : e * half + v_at].astype(f32)
            for g in range(4):
                moved = packed if g == 0 else pltpu.roll(packed, 128 - 32 * g, 1)
                lo = e * half_rows + g * eighth
                rotx[i, lo : lo + eighth] = moved.astype(bf16)

    def pieces(part, t=0):
        found = []
        for d, cc in ((2, 0), (2, 1), (1, 0), (3, 0), (1, 1), (3, 1), (0, 0)):
            dev = chip(d, cc) if d else partner
            slot = (0, 1, 3, 2)[d]
            src, dst = piece_refs(part, t, dev[1], slot)
            found.append(remote(src, dst, a_send.at[part + t, 2 * d + cc], a_recv.at[part + t, slot, core], dev))
        return found

    def piece_refs(part, t, owner, slot):
        if part == 0:
            return osw.at[pl.ds(pl.multiple_of(owner * mine, mine), mine)], orow.at[slot, core, 0]
        row_at = pl.multiple_of(t * QT + owner * sub, sub)
        there = pl.ds(pl.multiple_of(t * sub, sub), sub)
        return osl.at[pl.ds(row_at, sub)], orow.at[slot, core, 1, there]

    def piece_there(part, t, slot, cc):
        if part == 0:
            return orow.at[slot, cc, 0]
        return orow.at[slot, cc, 1, pl.ds(t * sub, sub)]

    S = ((s00, s01), (s10, s11), (s20, s21), (s30, s31))
    X = ((x00, x01), (x10, x11), (x20, x21), (x30, x31))

    def stage_a(k, q, t, slot, h):
        z64, z96 = jnp.zeros((64, QT), bf16), jnp.zeros((96, QT), bf16)
        keys = jnp.concatenate([kvb[k, 0:half_rows], kvb[k, half : half + half_rows]], axis=0)
        keys = jnp.concatenate([keys, rotx[k]], axis=1)
        qq = qb[q, t, h]
        parts = [z64, z64, qq[64:96], z96]
        parts[h] = qq[0:64]
        s = jnp.dot(keys, jnp.concatenate(parts, axis=0), preferred_element_type=f32)
        S[slot][h][...] = s
        X[slot][h][...] = jnp.max(s.reshape(rows // 8, 8, QT), axis=0)

    def stage_b(k, q, t, slot, h):
        old = mref[q, t, h : h + 1]
        new = jnp.maximum(old, jnp.max(X[slot][h][...], axis=0, keepdims=True))
        alpha = jnp.exp2(old - new)
        mref[q, t, h : h + 1] = new
        total = None
        for lo in range(0, rows, PV):
            hi = min(rows, lo + PV)
            p = jnp.exp2(S[slot][h][lo:hi] - new).astype(bf16)
            v_rows = [value_row(c) + 64 * h for c in range(lo, hi, 128)]
            v = jnp.concatenate([kvb[k, r : r + 64] for r in v_rows], axis=1)
            v = jnp.concatenate([v, jnp.ones((16, hi - lo), bf16)], axis=0)
            o = jnp.dot(v, p, preferred_element_type=f32)
            total = o if total is None else total + o
        lref[q, t, h : h + 1] = lref[q, t, h : h + 1] * alpha + total[64:65]
        acc[q, t, 64 * h : 64 * h + 64] = acc[q, t, 64 * h : 64 * h + 64] * alpha + total[0:64]

    def pipeline(n, where, before=None, after=None):
        def step(first, second):
            for i, _ in first:
                if before is not None:
                    before(i)
            for d in range(2):
                for h in range(2):
                    if d < len(first):
                        i, slot = first[d]
                        stage_a(*where(i), slot, h)
                    if d < len(second):
                        i, slot = second[d]
                        stage_b(*where(i), slot, h)
            for i, _ in second:
                if after is not None:
                    after(i)

        def body(i, at):
            step(
                [(i + 2, (at + 2) % 4), (i + 3, (at + 3) % 4)], [(i, at), (i + 1, at + 1)]
            )

        step([(0, 0), (1, 1)], [])
        bodies = n // 2 - 1
        loops = bodies // 2
        if loops == 1:
            body(0, 0)
            body(2, 2)
        elif loops:
            @pl.loop(0, loops)
            def _(j):
                body(4 * j, 0)
                body(4 * j + 2, 2)
        if bodies % 2:
            body(4 * loops, 0)
        i = 2 * bodies
        last = [(i, i % 4), (i + 1, (i + 1) % 4)]
        if n % 2:
            step([(i + 2, (i + 2) % 4)], last)
            last = [(i + 2, (i + 2) % 4)]
        step([], last)

    def window():
        for c in halo:
            c.wait_recv()
        span = QT + 2 * WINDOW
        key_i = lax.broadcasted_iota(jnp.int32, (span, QT), 0)
        dist = key_i - WINDOW - lax.broadcasted_iota(jnp.int32, (span, QT), 1)
        dist = jnp.abs(dist)
        distf = dist.astype(f32)

        @pl.loop(0, tiles)
        def _(t):
            rows_at = pl.ds(pl.multiple_of(t * QT, QT), span)
            kv = kvp[rows_at]
            pos = sp * rows + t * QT + key_i - WINDOW
            valid = (dist <= WINDOW) & (pos >= 0) & (pos < nsp * rows)
            for h in range(2):
                slope, sink = slopes[tp * 2 + h], sinks[h]
                rhs = jnp.concatenate([qwt[t, h], jnp.zeros((64, QT), bf16)], axis=0)
                s = jnp.dot(kv, rhs, preferred_element_type=f32) * 0.125
                s = jnp.where(valid, s - slope * distf, NEG)
                m = jnp.maximum(jnp.max(s, axis=0, keepdims=True), sink)
                w = jnp.exp2((s - m) * LOG2E)
                denom = jnp.sum(w, axis=0, keepdims=True) + jnp.exp2((sink - m) * LOG2E)
                w = (w * (1.0 / denom)).astype(bf16)
                o = lax.dot_general(kv, w, (((0,), (0,)), ((), ())), preferred_element_type=f32)
                S[0][0][h * 64 : h * 64 + 64] = o[64:128]
            osw[pl.ds(pl.multiple_of(t * QT, QT), QT), :] = S[0][0][0:128].T.astype(bf16)

    unpack(0)
    pipeline(tiles, lambda i: (0, 0, i))
    window()
    for c in pieces(0):
        c.start()
    orow[0, core, 0] = osw[pl.ds(pl.multiple_of(tp * mine, mine), mine), :]
    wts.first()

    def queries_arrive(i):
        if i % 2 == 0:
            t = i // 2
            q_out[(1, t)].wait_recv()
            q_out[(2, t)].wait_recv()
            for h in range(2):
                q_fwd[(t, h)].start()
            if t == tiles - 1:
                for c, f in ((k_out[(0, 0)], k_fwd[0]), (k_out[(1, 1)], k_fwd[1])):
                    c.wait_recv()
                    f.start()

    pipeline(2 * tiles, lambda i: (0, 1 + i % 2, i // 2), queries_arrive)

    unpack(1)
    pipeline(3 * tiles, lambda i: (1, i // tiles, i % tiles))
    k_out[(0, 1)].wait_recv()
    k_out[(1, 0)].wait_recv()
    unpack(2)
    for c in q_fwd.values():
        c.wait_recv()
    def arrive(i):
        @pl.when(i == 4 * tiles)
        def _():
            for c in k_fwd:
                c.wait_recv()
            unpack(3)

        @pl.when(i == 3 * tiles)
        def _():
            wts.second()

    def finish(q, t):
        for h in range(2):
            inv = 1.0 / lref[q, t, h : h + 1]
            osend[q, t, 64 * h : 64 * h + 64] = (acc[q, t, 64 * h : 64 * h + 64] * inv).astype(bf16)
        ssend[q, t, 0:2] = mref[q, t, 0:2]
        ssend[q, t, 2:4] = lref[q, t, 0:2]

    def back(q, t):
        slot, dev = {3: (3, zo), 2: (1, zr), 1: (2, zl)}[q]
        return (
            remote(osend.at[q, t], obuf.at[slot, t], o_send.at[q, t], o_recv.at[slot, t], dev),
            remote(ssend.at[q, t], sbuf.at[slot, t], s_send.at[q, t], s_recv.at[slot, t], dev),
        )

    def mixed_order(i):
        p = i // tiles
        return p - p // 3 - p // 5, 3 - p // 3 + p // 4 - p // 5, i % tiles

    def give_back(i):
        for q in (3, 2):
            @pl.when(i // tiles == 7 - q)
            def _():
                finish(q, i % tiles)
                for c in back(q, i % tiles):
                    c.start()

    pipeline(6 * tiles, mixed_order, arrive, give_back)

    def combine(t):
        for q in (3, 2, 1):
            for c in back(q, t):
                c.wait_recv()
        ms = [ssend[0, t, 0:2]] + [sbuf[j, t, 0:2] for j in (1, 2, 3)]
        ls = [ssend[0, t, 2:4]] + [sbuf[j, t, 2:4] for j in (1, 2, 3)]
        top = jnp.maximum(jnp.maximum(ms[0], ms[1]), jnp.maximum(ms[2], ms[3]))
        ws = [l * jnp.exp2(m - top) for m, l in zip(ms, ls)]
        inv = 1.0 / (ws[0] + ws[1] + ws[2] + ws[3])
        for h in range(2):
            rows_h = slice(64 * h, 64 * h + 64)
            total = osend[0, t, rows_h].astype(f32) * (ws[0] * inv)[h : h + 1]
            for j in (1, 2, 3):
                total = total + obuf[j, t, rows_h].astype(f32) * (ws[j] * inv)[h : h + 1]
            facc[rows_h] = total
        osl[pl.ds(pl.multiple_of(t * QT, QT), QT), :] = facc[...].T.astype(bf16)
        for c in pieces(1, t):
            c.start()
        src, dst = piece_refs(1, t, tp, 0)
        dst[...] = src[...]

    def by_tile(i):
        return 2 + i % 2, 1 - i // (2 * tiles), (i % (2 * tiles)) // 2

    def give_back_last(i):
        @pl.when(i % 2 == 1)
        def _():
            _, q, t = by_tile(i)
            finish(q, t)

            @pl.when(i < 2 * tiles)
            def _():
                for c in back(1, t):
                    c.start()

            @pl.when(i >= 2 * tiles)
            def _():
                combine(t)

    def late(i):
        @pl.when(i == 2 * tiles)
        def _():
            wts.third()

    pipeline(4 * tiles, by_tile, late, give_back_last)

    wts.fourth()
    def weights_there(slots):
        for s in slots:
            for p in (0, 1):
                wts.partner(s, p)

    def heads_there(parts):
        for part in parts:
            for s in range(4):
                for cc in (0, 1) if s else (1 - core,):
                    there = piece_there(min(part, 1), part - 1, s, cc)
                    remote(there, there, a_send.at[part, 0], a_recv.at[part, s, cc], partner).wait_recv()

    weights_there(range(4))
    heads_there(range(1 + tiles))
    stores = [
        pltpu.make_async_copy(
            total_out.at[:, pl.ds(b * CB, CB)], result.at[:, pl.ds(b * CB, CB)], r_sem.at[b]
        )
        for b in range(D // CB)
    ]
    for b, store in enumerate(stores):
        cols = pl.ds(b * CB, CB)
        total = None
        for s in range(4):
            for cc in (0, 1):
                o = jnp.concatenate([orow[s, cc, 0], orow[s, cc, 1]], axis=1)
                w = jnp.concatenate([wb[s, cc, 0, :, cols], wb[s, cc, 1, :, cols]], axis=0)
                g = jnp.dot(o, w, preferred_element_type=f32).astype(bf16).astype(f32)
                total = g if total is None else total + g
        total_out[:, cols] = total.astype(bf16)
        store.start()

    for c in halo + list(q_out.values()) + list(k_out.values()) + list(q_fwd.values()) + k_fwd:
        c.wait_send()
    for q in (3, 2, 1):
        for t in range(tiles):
            for c in back(q, t):
                c.wait_send()
    for c in pieces(0):
        c.wait_send()
    for t in range(tiles):
        for c in pieces(1, t):
            c.wait_send()
    tok.drain()
    wts.drain()
    for store in stores:
        store.wait()


def angle_tables(rows, nsp):
    inverse = THETA ** (-np.arange(16, dtype=np.float64) / 16)
    far = np.arange(nsp)[:, None] * rows * inverse[None, :]
    far = np.concatenate([np.cos(far), np.sin(far)], axis=1)[:, :, None]
    near = inverse[:, None] * np.arange(rows)[None, :]
    near = np.concatenate([np.cos(near), np.sin(near)], axis=0)
    return np.broadcast_to(far, (nsp, 32, 128)).astype(np.float32), near.astype(np.float32)


def per_device(
    nsp, ntp, tokens, norm_gain, window_query, window_key, window_value, sink_logit, down_query,
    down_latent, rotary_proj, query_gain, latent_gain, up_query, up_key, up_value, window_out, latent_out,
):
    rows = tokens.shape[0]
    tiles, mine, half_rows = rows // QT, rows // ntp, rows // 2
    far, near = angle_tables(rows, nsp)
    slopes = np.exp2(-8.0 * (np.arange(A_HEADS) + 1.0) / A_HEADS).astype(np.float32)
    dma, V = pltpu.SemaphoreType.DMA, pltpu.VMEM
    vm, smem = pl.BlockSpec(memory_space=pltpu.VMEM), pl.BlockSpec(memory_space=pltpu.SMEM)
    hbm = pl.BlockSpec(memory_space=pl.ANY)
    gather_sems = [dma((3, 2)), dma((4, 2)), dma((3,)), dma((4, 2)), dma((4, 2))]
    message = rows + rows // 4 + rows
    return pl.pallas_call(
        functools.partial(layer_kernel, rows, nsp // NX, NX, ntp // 2),
        out_shape=jax.ShapeDtypeStruct((mine, D), bf16),
        in_specs=[vm, vm, vm, vm, smem, smem] + [hbm] * 14,
        out_specs=hbm,
        scratch_shapes=[
            V((4, 2, 2, half_rows, 256), bf16), V((4, 2, 2, 128, D), bf16),
            V((D, 768), bf16), V((D, 512), bf16), V((D, 384), bf16),
            V((256, D), bf16),
            V((192, 768), bf16), V((512, 128), bf16), V((512, 128), bf16),
            V((32, 128), f32), V((32, rows), f32), V((32, rows), f32), V((rows, 1664), f32), V((rows, 128), f32),
            V((message, 128), bf16), V((tiles, 2, 64, QT), bf16), V((rows, 128), bf16),
            V((rows, 128), bf16), V((rows, 128), bf16), V((4, 2, 2, mine, 128), bf16),
            V((4, message, 128), bf16), V((4, rows, 128), bf16), V((4, tiles, 2, 96, QT), bf16),
            V((rows + 2 * WINDOW, 128), bf16),
            V((4, tiles, 8, QT), f32), V((4, tiles, 8, QT), f32), V((4, tiles, 128, QT), f32),
        ]
        + [V((rows, QT), f32)] * 8 + [V((8, QT), f32)] * 8 + [V((128, QT), f32), V((mine, D), bf16)]
        + [
            V((4, tiles, 128, QT), bf16), V((4, tiles, 8, QT), f32),
            V((4, tiles, 128, QT), bf16), V((4, tiles, 8, QT), f32),
            dma((14,)),
        ]
        + gather_sems
        + [dma((3, 3)), dma((3, 3)), dma((2,)), dma((2,)), dma((1,)), dma((1,)), dma((4, 2)), dma((4, 2))]
        + [
            dma((1 + tiles, 8)), dma((1 + tiles, 4, 2)), dma((D // CB,)),
            dma((2,)), dma((2,)), dma((3, tiles)), dma((3, tiles)), dma((tiles, 2)), dma((tiles, 2)),
            dma((2, 2)), dma((2, 2)), dma((2,)), dma((2,)),
            dma((4, tiles)), dma((4, tiles)), dma((4, tiles)), dma((4, tiles)),
        ],
        compiler_params=pltpu.CompilerParams(
            collective_id=1, has_side_effects=True, vmem_limit_bytes=60 * 2**20
        ),
        name="layer",
    )(
        tokens, norm_gain.reshape(1, D), query_gain.reshape(6, 128), latent_gain.reshape(1, -1),
        sink_logit, jnp.asarray(slopes), window_query, window_key.T, window_value.T, down_query, down_latent,
        rotary_proj.T, up_query.T, up_key, up_value, window_out, latent_out, jnp.asarray(far), jnp.asarray(near),
        jnp.asarray(near.reshape(32, ntp, tiles, mine // tiles).transpose(0, 2, 1, 3).reshape(32, rows)),
    )


def solution(mesh):
    col, row, rep = P(None, "tp"), P("tp", None), P()
    placed = (
        P("sp", "tp"), rep, col, col, col, P("tp"), rep, rep, rep, rep, rep, col, col, col, row, row,
    )
    body = functools.partial(per_device, mesh.shape["sp"], mesh.shape["tp"])
    return jax.shard_map(
        body, mesh=mesh, in_specs=placed, out_specs=P(("sp", "tp"), None), check_vma=False
    )
```

```python
import functools
import jax
import jax.numpy as jnp
import numpy as np
from jax import lax
from jax.experimental import pallas as pl
from jax.experimental.pallas import tpu as pltpu
from jax.sharding import PartitionSpec as P

D = 2048
A_HEADS = 16
WINDOW = 128
EPS = 1e-06
THETA = 10000.0
LOG2E = 1.4426950408889634
f32, bf16 = jnp.float32, jnp.bfloat16
MESH = pl.DeviceIdType.MESH
QT = 256
NEG = -1e30
NX = 4
PV = 768
CB = 512


def remote(src, dst, ss, rs, dev):
    return pltpu.make_async_remote_copy(
        src_ref=src, dst_ref=dst, send_sem=ss, recv_sem=rs, device_id=dev, device_id_type=MESH
    )


class ChipGather:
    def __init__(self, own, buf, core, right, left, partner, sems, keep):
        ysend, yrecv, fsend, psend, precv = sems
        self.own, self.buf, self.core = own, buf, core
        size = buf.shape[3]
        head, rest = pl.ds(0, keep), pl.ds(keep, size - keep)
        self.out = {
            (s, p): remote(own[p], buf.at[s, core, p], ysend.at[s, p], yrecv.at[s, p], dev)
            for s, dev in ((1, right), (2, left))
            for p in (0, 1)
        }
        self.fwd = {
            (3, 0): remote(
                buf.at[1, core, 0, head], buf.at[3, core, 0, head], fsend.at[0], yrecv.at[3, 0], right
            ),
            (3, 1): remote(buf.at[2, core, 1], buf.at[3, core, 1], fsend.at[1], yrecv.at[3, 1], left),
        }
        self.more = []
        if keep < size:
            self.more = [
                remote(buf.at[2, core, 0, rest], buf.at[3, core, 0, rest], fsend.at[2], yrecv.at[0, 0], left)
            ]
        self.relay = {
            (s, p): remote(
                own[p] if s == 0 else buf.at[s, core, p], buf.at[s, core, p],
                psend.at[s, p], precv.at[s, p], partner,
            )
            for s in range(4)
            for p in (0, 1)
        }

    def start(self):
        for key in ((1, 0), (2, 1), (1, 1), (2, 0)):
            self.out[key].start()
        for p in (0, 1):
            self.relay[(0, p)].start()

    def arrive(self, slot, part, relay=True):
        (self.fwd if slot == 3 else self.out)[(slot, part)].wait_recv()
        if (slot, part) == (1, 0):
            self.fwd[(3, 0)].start()
        if (slot, part) == (2, 1):
            self.fwd[(3, 1)].start()
        if (slot, part) == (2, 0):
            for c in self.more:
                c.start()
        if (slot, part) == (3, 0):
            for c in self.more:
                c.wait_recv()
        if relay:
            self.relay[(slot, part)].start()

    def partner(self, slot, part):
        self.relay[(slot, part)].wait_recv()

    def drain(self):
        for c in list(self.out.values()) + list(self.fwd.values()) + self.more + list(self.relay.values()):
            c.wait_send()


class WeightGather:
    def __init__(self, buf, core, a, right, left, partner, across, sems):
        osend, orecv, fsend, frecv, xsend, xrecv, psend, precv = sems
        rows = buf.shape[3]
        b, cut, mid = 1 - a, rows // 4, rows // 2
        chunks = ((a, pl.ds(0, rows)), (b, pl.ds(0, cut)), (b, pl.ds(cut, rows - cut)))
        self.out = {
            (s, i): remote(
                buf.at[0, core, p, r], buf.at[s, core, p, r], osend.at[s, i], orecv.at[s, i], dev
            )
            for s, dev in ((1, right), (2, left))
            for i, (p, r) in enumerate(chunks)
        }
        self.fwd = [
            remote(buf.at[s, core, a, r], buf.at[3, core, a, r], fsend.at[i], frecv.at[i], dev)
            for i, (s, dev, r) in enumerate(((1, right, pl.ds(0, mid)), (2, left, pl.ds(mid, rows - mid))))
        ]
        self.swap = remote(buf.at[3, core, a], buf.at[3, core, a], xsend.at[0], xrecv.at[0], across)
        self.relay = {
            (s, i): remote(
                buf.at[s, core, p], buf.at[s, core, p], psend.at[s, i], precv.at[s, i], partner
            )
            for s in range(4)
            for i, p in enumerate((a, b))
        }

    def start(self):
        for key in ((1, 0), (2, 0), (1, 1), (2, 1)):
            self.out[key].start()
        for i in (0, 1):
            self.relay[(0, i)].start()

    def first(self):
        for s in (1, 2):
            self.out[(s, 0)].wait_recv()
            self.fwd[s - 1].start()
        for s in (1, 2):
            self.out[(s, 2)].start()
            self.relay[(s, 0)].start()

    def second(self):
        for c in self.fwd:
            c.wait_recv()
        self.swap.start()
        self.relay[(3, 0)].start()

    def third(self):
        for s in (1, 2):
            self.out[(s, 1)].wait_recv()
            self.out[(s, 2)].wait_recv()
            self.relay[(s, 1)].start()

    def fourth(self):
        self.swap.wait_recv()
        self.relay[(3, 1)].start()

    def partner(self, slot, part):
        self.relay[(slot, part)].wait_recv()

    def drain(self):
        for c in list(self.out.values()) + self.fwd + [self.swap] + list(self.relay.values()):
            c.wait_send()


def layer_kernel(
    rows, nz, nx, ny,
    tokens, norm_gain, query_gain, latent_gain, sinks, slopes,
    w_query, w_key, w_value, d_query, d_latent, w_rot, u_query, u_key, u_value, o_window, o_latent,
    tab_far, tab_near, tab_near_q,
    result,
    tb, wb, wdq, wdl, wcat, wnarrow, uq, uk, uv, far, near, near_q, pacc, sq,
    kvm, qwt, kvw, osw, osl, orow,
    kvb, rotx, qb, kvp, mref, lref, acc,
    s00, s01, s10, s11, s20, s21, s30, s31, x00, x01, x10, x11, x20, x21, x30, x31, facc, total_out,
    osend, ssend, obuf, sbuf,
    l_sem, t_ysend, t_yrecv, t_fsend, t_psend, t_precv, w_osend, w_orecv, w_fsend, w_frecv, w_xsend, w_xrecv, w_psend, w_precv,
    a_send, a_recv, r_sem,
    h_send, h_recv, q_send, q_recv, qf_send, qf_recv, k_send, k_recv, kf_send, kf_recv,
    o_send, o_recv, s_send, s_recv,
):
    sp = lax.axis_index("sp")
    tp = lax.axis_index("tp")
    z, x = sp // nx, sp % nx
    y, core = tp // 2, tp % 2
    nsp, ntp = nz * nx, ny * 2
    tiles = rows // QT
    half_rows = rows // 2
    mine = rows // ntp

    loads = [
        pltpu.make_async_copy(s, d, l_sem.at[i])
        for i, (s, d) in enumerate((
            (d_query, wdq), (d_latent, wdl), (w_query, wcat.at[:, pl.ds(0, 128)]),
            (w_key, wnarrow.at[pl.ds(0, 64)]), (w_value, wnarrow.at[pl.ds(64, 64)]),
            (w_rot, wnarrow.at[pl.ds(128, 32)]), (u_query, uq), (u_key, uk), (u_value, uv),
            (tab_far.at[sp], far), (tab_near, near), (tab_near_q, near_q),
            (o_window, wb.at[0, core, 0]), (o_latent, wb.at[0, core, 1]),
        ))
    ]
    for c in loads:
        c.start()

    def at(zz, xx):
        return (zz * nx + xx, tp)

    def chip(step, cc):
        return (sp, ((y + step) % ny) * 2 + cc)

    xr, xl = at(z, (x + 1) % nx), at(z, (x + nx - 1) % nx)
    zr, zl, zo = at((z + 1) % nz, x), at((z + nz - 1) % nz, x), at((z + 2) % nz, x)
    nxt, prv = ((sp + 1) % nsp, tp), ((sp + nsp - 1) % nsp, tp)
    partner = chip(0, 1 - core)
    others = [chip(d, cc) for d in range(1, ny) for cc in (0, 1)] + [partner]

    barrier = pltpu.get_barrier_semaphore()
    peers = [xr, xl, zr, zl, zo, nxt, prv] + others
    for peer in peers:
        pl.semaphore_signal(barrier, inc=1, device_id=peer, device_id_type=MESH)
    pl.semaphore_wait(barrier, len(peers))

    tok = ChipGather(
        [tokens.at[pl.ds(p * half_rows, half_rows)] for p in (0, 1)], tb, core,
        chip(1, core), chip(ny - 1, core), partner, (t_ysend, t_yrecv, t_fsend, t_psend, t_precv), half_rows,
    )
    wts = WeightGather(
        wb, core, x % 2, chip(1, core), chip(ny - 1, core), partner, at(z, x + 1 - 2 * (x % 2)),
        (w_osend, w_orecv, w_fsend, w_frecv, w_xsend, w_xrecv, w_psend, w_precv),
    )
    tok.start()
    for p in (0, 1):
        tb[0, core, p] = tokens[p * half_rows : (p + 1) * half_rows]

    mref[...] = jnp.full(mref.shape, NEG, f32)
    lref[...] = jnp.zeros(lref.shape, f32)
    acc[...] = jnp.zeros(acc.shape, f32)
    ssend[...] = jnp.zeros(ssend.shape, f32)
    pacc[...] = jnp.zeros(pacc.shape, f32)
    sq[...] = jnp.zeros(sq.shape, f32)
    wnarrow[160:256] = jnp.zeros((96, D), bf16)
    for c in loads:
        c.wait()

    @pl.loop(0, D // 128)
    def _(b):
        at_b = pl.ds(pl.multiple_of(b * 128, 128), 128)
        wcat[at_b, 128:384] = wnarrow[:, at_b].astype(f32).T.astype(bf16)

    arrivals = {(1, 0): ((1, 0), (2, 1)), (1, 1): ((1, 1), (2, 0))}

    all_parts = ((wdl, 768, 1280), (wcat, 1280, 1664), (wdq, 0, 768))

    def unit(t32, w_rows, out_rows, parts=all_parts, count=True):
        if count:
            squares = t32 * t32
            part_sq = squares[:, 0:128]
            for lo in range(128, t32.shape[1], 128):
                part_sq = part_sq + squares[:, lo : lo + 128]
            sq[out_rows] += part_sq
        scaled = (t32 * norm_gain[:, w_rows]).astype(bf16)
        for w, lo, hi in parts:
            pacc[out_rows, lo:hi] += jnp.dot(scaled, w[w_rows, :], preferred_element_type=f32)

    @pl.loop(0, 3)
    def _(slot):
        chip_at = (y + ny - (slot + slot // 2)) % ny
        w_rows = pl.ds(pl.multiple_of(chip_at * 512, 512), 512)

        @pl.loop(0, 2)
        def _(part):
            for s in range(3):
                for p in (0, 1):
                    @pl.when((slot == s) & (part == p))
                    def _():
                        for key in arrivals.get((s, p), ()):
                            tok.arrive(*key)
                        if (s, p) == (1, 1):
                            wts.start()
                        tok.partner(s, p)
            out_rows = pl.ds(pl.multiple_of(part * half_rows, half_rows), half_rows)
            t32 = jnp.concatenate([tb[slot, 0, part], tb[slot, 1, part]], axis=1).astype(f32)
            unit(t32, w_rows, out_rows)

    tok.arrive(3, 0)
    tok.arrive(3, 1)

    @pl.loop(0, 2)
    def _(turn):
        from_core = core + turn - 2 * core * turn

        @pl.when(turn == 1)
        def _():
            tok.partner(3, 0)
            tok.partner(3, 1)

        @pl.loop(0, 2)
        def _(part):
            w_rows = pl.ds(pl.multiple_of(((y + 2) % ny) * 512 + from_core * 256, 256), 256)
            out_rows = pl.ds(pl.multiple_of(part * half_rows, half_rows), half_rows)
            unit(tb[3, from_core, part].astype(f32), w_rows, out_rows, all_parts[:2])

    cos_f, sin_f = far[0:16, 0:1], far[16:32, 0:1]
    for table in (near, near_q):
        cos_n, sin_n = table[0:16, :], table[16:32, :]
        cos, sin = cos_f * cos_n - sin_f * sin_n, sin_f * cos_n + cos_f * sin_n
        table[0:16, :] = cos
        table[16:32, :] = sin
    row_scale = lax.rsqrt(jnp.sum(sq[...], axis=1, keepdims=True) * (1.0 / D) + EPS)

    def normed(lo, hi, gain):
        v = (pacc[:, lo:hi] * row_scale).astype(bf16).astype(f32)
        scale = lax.rsqrt(jnp.sum(v * v, axis=1, keepdims=True) * (1.0 / (hi - lo)) + EPS)
        return (v * scale * gain).astype(bf16)

    kvw[...] = (pacc[:, 1408:1536] * row_scale).astype(bf16)
    halo = [
        remote(kvw.at[pl.ds(rows - WINDOW, WINDOW)], kvp.at[pl.ds(0, WINDOW)], h_send.at[0], h_recv.at[0], nxt),
        remote(kvw.at[pl.ds(0, WINDOW)], kvp.at[pl.ds(rows + WINDOW, WINDOW)], h_send.at[1], h_recv.at[1], prv),
    ]
    for c in halo:
        c.start()
    quarter, eighth = rows // 4, rows // 8
    half = kvm.shape[0] // 2
    v_at = half_rows + eighth

    def value_row(c):
        return (c // half_rows) * half + v_at + c % half_rows

    up_kv = jnp.concatenate([uk[...], uv[...]], axis=1)
    kv = jnp.dot(normed(768, 1280, latent_gain[...]), up_kv, preferred_element_type=f32)
    for e in (0, 1):
        kvm[e * half : e * half + half_rows] = kv[e * half_rows : (e + 1) * half_rows, 0:128].astype(bf16)
    for b in range(rows // 128):
        block = kv[128 * b : 128 * b + 128, 128:256].T
        kvm[value_row(128 * b) : value_row(128 * b) + 128] = block.astype(bf16)
    rr = (pacc[:, 1536:1664] * row_scale).astype(bf16).astype(f32).T
    ra, rb = rr[0:16], rr[16:32]
    cos, sin = near[0:16, :], near[16:32, :]
    turned = jnp.concatenate([ra * cos - rb * sin, rb * cos + ra * sin, jnp.zeros((96, rows), f32)], axis=0).T
    for e in (0, 1):
        packed = turned[e * half_rows : e * half_rows + eighth]
        for g in range(1, 4):
            lo = e * half_rows + g * eighth
            packed = packed + pltpu.roll(turned[lo : lo + eighth], 32 * g, 1)
        kvm[e * half + half_rows : e * half + v_at] = packed.astype(bf16)
    k_out = {}
    for order in ((0, 1), (1, 0)):
        for which, h in ((0, order[0]), (1, order[1])):
            slot, dev = 1 if which == h else 2, (xr, xl)[which]
            k_out[(which, h)] = remote(
                kvm.at[pl.ds(h * half, half)], kvb.at[slot, pl.ds(h * half, half)],
                k_send.at[which, h], k_recv.at[which, h], dev,
            )
    for key in ((0, 0), (1, 1), (0, 1), (1, 0)):
        k_out[key].start()
    kvb[0] = kvm[...]

    @pl.loop(0, 2)
    def _(part):
        w_rows = pl.ds(pl.multiple_of(((y + 2) % ny) * 512, 512), 512)
        out_rows = pl.ds(pl.multiple_of(part * half_rows, half_rows), half_rows)
        t32 = jnp.concatenate([tb[3, 0, part], tb[3, 1, part]], axis=1).astype(f32)
        unit(t32, w_rows, out_rows, all_parts[2:], False)

    sub = mine // tiles
    nq = normed(0, 768, jnp.concatenate([query_gain[i : i + 1] for i in range(6)], axis=1))
    nq = jnp.concatenate(
        [nq[mine * j + sub * t : mine * j + sub * t + sub] for t in range(tiles) for j in range(ntp)], axis=0
    )
    qf = lax.dot_general(uq[...], nq, (((1,), (1,)), ((), ())), preferred_element_type=f32) * (LOG2E * 96 ** (-0.5))
    cos, sin = near_q[0:16, :], near_q[16:32, :]
    for h in range(2):
        a, b = qf[96 * h + 64 : 96 * h + 80], qf[96 * h + 80 : 96 * h + 96]
        whole = jnp.concatenate(
            [qf[96 * h : 96 * h + 64], a * cos - b * sin, b * cos + a * sin], axis=0
        ).astype(bf16)
        for t in range(tiles):
            qb[0, t, h] = whole[:, QT * t : QT * t + QT]
    q_out = {
        (slot, t): remote(qb.at[0, t], qb.at[slot, t], q_send.at[slot, t], q_recv.at[slot, t], dev)
        for t in range(tiles)
        for slot, dev in ((1, zr), (2, zl))
    }
    for c in q_out.values():
        c.start()
    q_fwd = {}
    for n in range(2 * tiles):
        t, h = n // 2, n % 2
        slot, dev = (1, zr) if n < tiles else (2, zl)
        q_fwd[(t, h)] = remote(qb.at[slot, t, h], qb.at[3, t, h], qf_send.at[t, h], qf_recv.at[t, h], dev)

    kvp[WINDOW : WINDOW + rows] = kvw[...]
    wq = pacc[:, 1280:1408] * row_scale
    for t in range(tiles):
        qwt[t] = wq[QT * t : QT * t + QT].T.astype(bf16).reshape(2, 64, QT)
    k_fwd = [
        remote(kvb.at[1, pl.ds(0, half)], kvb.at[3, pl.ds(0, half)], kf_send.at[0], kf_recv.at[0], xr),
        remote(kvb.at[1, pl.ds(half, half)], kvb.at[3, pl.ds(half, half)], kf_send.at[1], kf_recv.at[1], xl),
    ]

    def unpack(i):
        for e in (0, 1):
            packed = kvb[i, e * half + half_rows : e * half + v_at].astype(f32)
            for g in range(4):
                moved = packed if g == 0 else pltpu.roll(packed, 128 - 32 * g, 1)
                lo = e * half_rows + g * eighth
                rotx[i, lo : lo + eighth] = moved.astype(bf16)

    def pieces(part, t=0):
        found = []
        for d, cc in ((2, 0), (2, 1), (1, 0), (3, 0), (1, 1), (3, 1), (0, 0)):
            dev = chip(d, cc) if d else partner
            slot = (0, 1, 3, 2)[d]
            src, dst = piece_refs(part, t, dev[1], slot)
            found.append(remote(src, dst, a_send.at[part + t, 2 * d + cc], a_recv.at[part + t, slot, core], dev))
        return found

    def piece_refs(part, t, owner, slot):
        if part == 0:
            return osw.at[pl.ds(pl.multiple_of(owner * mine, mine), mine)], orow.at[slot, core, 0]
        row_at = pl.multiple_of(t * QT + owner * sub, sub)
        there = pl.ds(pl.multiple_of(t * sub, sub), sub)
        return osl.at[pl.ds(row_at, sub)], orow.at[slot, core, 1, there]

    def piece_there(part, t, slot, cc):
        if part == 0:
            return orow.at[slot, cc, 0]
        return orow.at[slot, cc, 1, pl.ds(t * sub, sub)]

    S = ((s00, s01), (s10, s11), (s20, s21), (s30, s31))
    X = ((x00, x01), (x10, x11), (x20, x21), (x30, x31))

    def stage_a(k, q, t, slot, h):
        z64, z96 = jnp.zeros((64, QT), bf16), jnp.zeros((96, QT), bf16)
        keys = jnp.concatenate([kvb[k, 0:half_rows], kvb[k, half : half + half_rows]], axis=0)
        keys = jnp.concatenate([keys, rotx[k]], axis=1)
        qq = qb[q, t, h]
        parts = [z64, z64, qq[64:96], z96]
        parts[h] = qq[0:64]
        s = jnp.dot(keys, jnp.concatenate(parts, axis=0), preferred_element_type=f32)
        S[slot][h][...] = s
        X[slot][h][...] = jnp.max(s.reshape(rows // 8, 8, QT), axis=0)

    def stage_b(k, q, t, slot, h):
        old = mref[q, t, h : h + 1]
        new = jnp.maximum(old, jnp.max(X[slot][h][...], axis=0, keepdims=True))
        alpha = jnp.exp2(old - new)
        mref[q, t, h : h + 1] = new
        total = None
        for lo in range(0, rows, PV):
            hi = min(rows, lo + PV)
            p = jnp.exp2(S[slot][h][lo:hi] - new).astype(bf16)
            v_rows = [value_row(c) + 64 * h for c in range(lo, hi, 128)]
            v = jnp.concatenate([kvb[k, r : r + 64] for r in v_rows], axis=1)
            v = jnp.concatenate([v, jnp.ones((16, hi - lo), bf16)], axis=0)
            o = jnp.dot(v, p, preferred_element_type=f32)
            total = o if total is None else total + o
        lref[q, t, h : h + 1] = lref[q, t, h : h + 1] * alpha + total[64:65]
        acc[q, t, 64 * h : 64 * h + 64] = acc[q, t, 64 * h : 64 * h + 64] * alpha + total[0:64]

    def pipeline(n, where, before=None, after=None):
        def step(first, second):
            for i, _ in first:
                if before is not None:
                    before(i)
            for d in range(2):
                for h in range(2):
                    if d < len(first):
                        i, slot = first[d]
                        stage_a(*where(i), slot, h)
                    if d < len(second):
                        i, slot = second[d]
                        stage_b(*where(i), slot, h)
            for i, _ in second:
                if after is not None:
                    after(i)

        def body(i, at):
            step(
                [(i + 2, (at + 2) % 4), (i + 3, (at + 3) % 4)], [(i, at), (i + 1, at + 1)]
            )

        step([(0, 0), (1, 1)], [])
        bodies = n // 2 - 1
        loops = bodies // 2
        if loops == 1:
            body(0, 0)
            body(2, 2)
        elif loops:
            @pl.loop(0, loops)
            def _(j):
                body(4 * j, 0)
                body(4 * j + 2, 2)
        if bodies % 2:
            body(4 * loops, 0)
        i = 2 * bodies
        last = [(i, i % 4), (i + 1, (i + 1) % 4)]
        if n % 2:
            step([(i + 2, (i + 2) % 4)], last)
            last = [(i + 2, (i + 2) % 4)]
        step([], last)

    def window():
        for c in halo:
            c.wait_recv()
        span = QT + 2 * WINDOW
        key_i = lax.broadcasted_iota(jnp.int32, (span, QT), 0)
        dist = key_i - WINDOW - lax.broadcasted_iota(jnp.int32, (span, QT), 1)
        dist = jnp.abs(dist)
        distf = dist.astype(f32)

        @pl.loop(0, tiles)
        def _(t):
            rows_at = pl.ds(pl.multiple_of(t * QT, QT), span)
            kv = kvp[rows_at]
            pos = sp * rows + t * QT + key_i - WINDOW
            valid = (dist <= WINDOW) & (pos >= 0) & (pos < nsp * rows)
            for h in range(2):
                slope, sink = slopes[tp * 2 + h], sinks[h]
                rhs = jnp.concatenate([qwt[t, h], jnp.zeros((64, QT), bf16)], axis=0)
                s = jnp.dot(kv, rhs, preferred_element_type=f32) * 0.125
                s = jnp.where(valid, s - slope * distf, NEG)
                m = jnp.maximum(jnp.max(s, axis=0, keepdims=True), sink)
                w = jnp.exp2((s - m) * LOG2E)
                denom = jnp.sum(w, axis=0, keepdims=True) + jnp.exp2((sink - m) * LOG2E)
                w = (w * (1.0 / denom)).astype(bf16)
                o = lax.dot_general(kv, w, (((0,), (0,)), ((), ())), preferred_element_type=f32)
                S[0][0][h * 64 : h * 64 + 64] = o[64:128]
            osw[pl.ds(pl.multiple_of(t * QT, QT), QT), :] = S[0][0][0:128].T.astype(bf16)

    unpack(0)
    pipeline(tiles, lambda i: (0, 0, i))
    window()
    for c in pieces(0):
        c.start()
    orow[0, core, 0] = osw[pl.ds(pl.multiple_of(tp * mine, mine), mine), :]
    wts.first()

    def queries_arrive(i):
        if i % 2 == 0:
            t = i // 2
            q_out[(1, t)].wait_recv()
            q_out[(2, t)].wait_recv()
            for h in range(2):
                q_fwd[(t, h)].start()
            if t == tiles - 1:
                for c, f in ((k_out[(0, 0)], k_fwd[0]), (k_out[(1, 1)], k_fwd[1])):
                    c.wait_recv()
                    f.start()

    pipeline(2 * tiles, lambda i: (0, 1 + i % 2, i // 2), queries_arrive)

    unpack(1)
    pipeline(3 * tiles, lambda i: (1, i // tiles, i % tiles))
    k_out[(0, 1)].wait_recv()
    k_out[(1, 0)].wait_recv()
    unpack(2)
    for c in q_fwd.values():
        c.wait_recv()
    def arrive(i):
        @pl.when(i == 3 * tiles)
        def _():
            for c in k_fwd:
                c.wait_recv()
            unpack(3)

        @pl.when(i == 3 * tiles)
        def _():
            wts.second()

    def finish(q, t):
        for h in range(2):
            inv = 1.0 / lref[q, t, h : h + 1]
            osend[q, t, 64 * h : 64 * h + 64] = (acc[q, t, 64 * h : 64 * h + 64] * inv).astype(bf16)
        ssend[q, t, 0:2] = mref[q, t, 0:2]
        ssend[q, t, 2:4] = lref[q, t, 0:2]

    def back(q, t):
        slot, dev = {3: (3, zo), 2: (1, zr), 1: (2, zl)}[q]
        return (
            remote(osend.at[q, t], obuf.at[slot, t], o_send.at[q, t], o_recv.at[slot, t], dev),
            remote(ssend.at[q, t], sbuf.at[slot, t], s_send.at[q, t], s_recv.at[slot, t], dev),
        )

    def mixed_order(i):
        p = i // tiles
        return p - 2 * (p // 4), 3 - p // 4, i % tiles

    def give_back(i):
        for q in (3, 2):
            @pl.when(i // tiles == 9 - 2 * q)
            def _():
                finish(q, i % tiles)
                for c in back(q, i % tiles):
                    c.start()

    pipeline(6 * tiles, mixed_order, arrive, give_back)

    def combine(t):
        for q in (3, 2, 1):
            for c in back(q, t):
                c.wait_recv()
        ms = [ssend[0, t, 0:2]] + [sbuf[j, t, 0:2] for j in (1, 2, 3)]
        ls = [ssend[0, t, 2:4]] + [sbuf[j, t, 2:4] for j in (1, 2, 3)]
        top = jnp.maximum(jnp.maximum(ms[0], ms[1]), jnp.maximum(ms[2], ms[3]))
        ws = [l * jnp.exp2(m - top) for m, l in zip(ms, ls)]
        inv = 1.0 / (ws[0] + ws[1] + ws[2] + ws[3])
        for h in range(2):
            rows_h = slice(64 * h, 64 * h + 64)
            total = osend[0, t, rows_h].astype(f32) * (ws[0] * inv)[h : h + 1]
            for j in (1, 2, 3):
                total = total + obuf[j, t, rows_h].astype(f32) * (ws[j] * inv)[h : h + 1]
            facc[rows_h] = total
        osl[pl.ds(pl.multiple_of(t * QT, QT), QT), :] = facc[...].T.astype(bf16)
        for c in pieces(1, t):
            c.start()
        src, dst = piece_refs(1, t, tp, 0)
        dst[...] = src[...]

    def by_tile(i):
        return 2 + i % 2, 1 - i // (2 * tiles), (i % (2 * tiles)) // 2

    def give_back_last(i):
        @pl.when(i % 2 == 1)
        def _():
            _, q, t = by_tile(i)
            finish(q, t)

            @pl.when(i < 2 * tiles)
            def _():
                for c in back(1, t):
                    c.start()

            @pl.when(i >= 2 * tiles)
            def _():
                combine(t)

    def late(i):
        @pl.when(i == 2 * tiles)
        def _():
            wts.third()

    pipeline(4 * tiles, by_tile, late, give_back_last)

    wts.fourth()
    def weights_there(slots):
        for s in slots:
            for p in (0, 1):
                wts.partner(s, p)

    def heads_there(parts):
        for part in parts:
            for s in range(4):
                for cc in (0, 1) if s else (1 - core,):
                    there = piece_there(min(part, 1), part - 1, s, cc)
                    remote(there, there, a_send.at[part, 0], a_recv.at[part, s, cc], partner).wait_recv()

    weights_there(range(4))
    heads_there(range(1 + tiles))
    stores = [
        pltpu.make_async_copy(
            total_out.at[:, pl.ds(b * CB, CB)], result.at[:, pl.ds(b * CB, CB)], r_sem.at[b]
        )
        for b in range(D // CB)
    ]
    for b, store in enumerate(stores):
        cols = pl.ds(b * CB, CB)
        total = None
        for s in range(4):
            for cc in (0, 1):
                o = jnp.concatenate([orow[s, cc, 0], orow[s, cc, 1]], axis=1)
                w = jnp.concatenate([wb[s, cc, 0, :, cols], wb[s, cc, 1, :, cols]], axis=0)
                g = jnp.dot(o, w, preferred_element_type=f32).astype(bf16).astype(f32)
                total = g if total is None else total + g
        total_out[:, cols] = total.astype(bf16)
        store.start()

    for c in halo + list(q_out.values()) + list(k_out.values()) + list(q_fwd.values()) + k_fwd:
        c.wait_send()
    for q in (3, 2, 1):
        for t in range(tiles):
            for c in back(q, t):
                c.wait_send()
    for c in pieces(0):
        c.wait_send()
    for t in range(tiles):
        for c in pieces(1, t):
            c.wait_send()
    tok.drain()
    wts.drain()
    for store in stores:
        store.wait()


def angle_tables(rows, nsp):
    inverse = THETA ** (-np.arange(16, dtype=np.float64) / 16)
    far = np.arange(nsp)[:, None] * rows * inverse[None, :]
    far = np.concatenate([np.cos(far), np.sin(far)], axis=1)[:, :, None]
    near = inverse[:, None] * np.arange(rows)[None, :]
    near = np.concatenate([np.cos(near), np.sin(near)], axis=0)
    return np.broadcast_to(far, (nsp, 32, 128)).astype(np.float32), near.astype(np.float32)


def per_device(
    nsp, ntp, tokens, norm_gain, window_query, window_key, window_value, sink_logit, down_query,
    down_latent, rotary_proj, query_gain, latent_gain, up_query, up_key, up_value, window_out, latent_out,
):
    rows = tokens.shape[0]
    tiles, mine, half_rows = rows // QT, rows // ntp, rows // 2
    far, near = angle_tables(rows, nsp)
    slopes = np.exp2(-8.0 * (np.arange(A_HEADS) + 1.0) / A_HEADS).astype(np.float32)
    dma, V = pltpu.SemaphoreType.DMA, pltpu.VMEM
    vm, smem = pl.BlockSpec(memory_space=pltpu.VMEM), pl.BlockSpec(memory_space=pltpu.SMEM)
    hbm = pl.BlockSpec(memory_space=pl.ANY)
    gather_sems = [dma((3, 2)), dma((4, 2)), dma((3,)), dma((4, 2)), dma((4, 2))]
    message = rows + rows // 4 + rows
    return pl.pallas_call(
        functools.partial(layer_kernel, rows, nsp // NX, NX, ntp // 2),
        out_shape=jax.ShapeDtypeStruct((mine, D), bf16),
        in_specs=[vm, vm, vm, vm, smem, smem] + [hbm] * 14,
        out_specs=hbm,
        scratch_shapes=[
            V((4, 2, 2, half_rows, 256), bf16), V((4, 2, 2, 128, D), bf16),
            V((D, 768), bf16), V((D, 512), bf16), V((D, 384), bf16),
            V((256, D), bf16),
            V((192, 768), bf16), V((512, 128), bf16), V((512, 128), bf16),
            V((32, 128), f32), V((32, rows), f32), V((32, rows), f32), V((rows, 1664), f32), V((rows, 128), f32),
            V((message, 128), bf16), V((tiles, 2, 64, QT), bf16), V((rows, 128), bf16),
            V((rows, 128), bf16), V((rows, 128), bf16), V((4, 2, 2, mine, 128), bf16),
            V((4, message, 128), bf16), V((4, rows, 128), bf16), V((4, tiles, 2, 96, QT), bf16),
            V((rows + 2 * WINDOW, 128), bf16),
            V((4, tiles, 8, QT), f32), V((4, tiles, 8, QT), f32), V((4, tiles, 128, QT), f32),
        ]
        + [V((rows, QT), f32)] * 8 + [V((8, QT), f32)] * 8 + [V((128, QT), f32), V((mine, D), bf16)]
        + [
            V((4, tiles, 128, QT), bf16), V((4, tiles, 8, QT), f32),
            V((4, tiles, 128, QT), bf16), V((4, tiles, 8, QT), f32),
            dma((14,)),
        ]
        + gather_sems
        + [dma((3, 3)), dma((3, 3)), dma((2,)), dma((2,)), dma((1,)), dma((1,)), dma((4, 2)), dma((4, 2))]
        + [
            dma((1 + tiles, 8)), dma((1 + tiles, 4, 2)), dma((D // CB,)),
            dma((2,)), dma((2,)), dma((3, tiles)), dma((3, tiles)), dma((tiles, 2)), dma((tiles, 2)),
            dma((2, 2)), dma((2, 2)), dma((2,)), dma((2,)),
            dma((4, tiles)), dma((4, tiles)), dma((4, tiles)), dma((4, tiles)),
        ],
        compiler_params=pltpu.CompilerParams(
            collective_id=1, has_side_effects=True, vmem_limit_bytes=60 * 2**20
        ),
        name="layer",
    )(
        tokens, norm_gain.reshape(1, D), query_gain.reshape(6, 128), latent_gain.reshape(1, -1),
        sink_logit, jnp.asarray(slopes), window_query, window_key.T, window_value.T, down_query, down_latent,
        rotary_proj.T, up_query.T, up_key, up_value, window_out, latent_out, jnp.asarray(far), jnp.asarray(near),
        jnp.asarray(near.reshape(32, ntp, tiles, mine // tiles).transpose(0, 2, 1, 3).reshape(32, rows)),
    )


def solution(mesh):
    col, row, rep = P(None, "tp"), P("tp", None), P()
    placed = (
        P("sp", "tp"), rep, col, col, col, P("tp"), rep, rep, rep, rep, rep, col, col, col, row, row,
    )
    body = functools.partial(per_device, mesh.shape["sp"], mesh.shape["tp"])
    return jax.shard_map(
        body, mesh=mesh, in_specs=placed, out_specs=P(("sp", "tp"), None), check_vma=False
    )
```
